256 devices in a mesh: sp: 32 (over z, y), tp: 8 (over x, core).
Axes of the slice: x: 4, y: 4, z: 8, core: 2. Of those that a mesh axis runs over, the one named last changes fastest.
Arguments:
- head_value_rows: bfloat16 [24576, 2048], P('sp', 'tp'), may hold values from -6 to 6
- entry_map_rows: bfloat16 [24576, 1024], P('sp', 'tp'), may hold values from -6 to 6
- readout_map_rows: bfloat16 [24576, 1024], P('sp', 'tp'), may hold values from -6 to 6
- output_gate_rows: bfloat16 [24576, 2048], P('sp', 'tp'), may hold values from -6 to 6
- step_before_softplus: bfloat16 [24576, 32], P('sp', 'tp'), may hold values from -8 to 8
- sudden_log_decay: float32 [24576, 32], P('sp', 'tp'), may hold values from -1 to 0
- document_index: int32 [24576], replicated, may hold values from 0 to 7, never falling along the last dimension, each value on 1 to 6144 neighbouring positions
- head_rate_logarithm: float32 [2, 32], P(None, 'tp'), may hold values from -30 to 0
- head_step_bias: float32 [2, 32], P(None, 'tp'), may hold values from -3 to 3
- value_conv_taps: bfloat16 [5, 2048], P(None, 'tp'), may hold values from -2.5 to 2.5
- entry_conv_taps: bfloat16 [5, 1024], P(None, 'tp'), may hold values from -2.5 to 2.5
- readout_conv_taps: bfloat16 [5, 1024], P(None, 'tp'), may hold values from -2.5 to 2.5
- group_norm_gain: float32 [2048], P('tp'), may hold values from 0.1 to 1.9
- mixer_output_weight: bfloat16 [2048, 2048], P('tp'), may hold values from -0.125 to 0.125
- stream: bfloat16 [24576, 2048], P('sp', 'tp'), may hold values from -200 to 200
- mixer_norm_gain: float32 [2048], P('tp'), may hold values from 0.1 to 1.9
- channel_norm_gain: float32 [2048], P('tp'), may hold values from 0.1 to 1.9
- up_projection_weight: bfloat16 [2048, 8192], P('sp', 'tp'), may hold values from -0.125 to 0.125
- down_projection_weight: bfloat16 [2048, 8192], P('sp', 'tp'), may hold values from -0.0625 to 0.0625
Outputs:
- mixed: bfloat16 [24576, 2048], P('sp', 'tp')
The draws below stay inside these ranges and needn't reach their ends.
All inputs are finite; a program needn't handle non-finite values.
Results may differ from the reference program's by a relative error of at most 0.018.
Values may be sent and summed in bfloat16 or wider, within the bound.
No kernel may reach another device: no remote copies, remote signals or barrier semaphores. Data moves between devices by JAX's collectives and lax.ppermute only.
A program may use at most 64 MiB of HBM per device.

```python
import math
import jax
import jax.numpy as jnp
import numpy as np
from jax import lax

D = 2048
HEADS = 32
HEAD_DIM = 64
GROUPS = 8
STATE = 128
FF = 8192
CONV_WIDTH = 5
BLOCK = 128
TOK_DEV = 768
INNER = 2048
TOKENS = 24576
N_SP = 32
N_TP = 8


def draw_step_before_softplus(key, part):
    jitter_key, shift_key = jax.random.split(key)
    jitter = jnp.clip(jax.random.normal(jitter_key, (TOKENS, HEADS), jnp.float32), -4.0, 4.0)
    shifts = jax.random.uniform(shift_key, (TOKENS // TOK_DEV, 1, HEADS), jnp.float32, -1.0, 1.5)
    shifts = jnp.broadcast_to(shifts, (TOKENS // TOK_DEV, TOK_DEV, HEADS)).reshape(TOKENS, HEADS)
    return (jitter + shifts).astype(jnp.bfloat16)


def draw_head_rate_logarithm(key, part):
    pick_key, slow_key, fast_key = jax.random.split(key, 3)
    quick = jax.random.randint(pick_key, (2, HEADS), 0, 2) == 1
    slow_rate = jax.random.uniform(slow_key, (2, HEADS), jnp.float32, math.log(0.1), math.log(0.5))
    slow_rate = slow_rate - jnp.log(jnp.float32(TOKENS))
    fast_rate = jax.random.uniform(fast_key, (2, HEADS), jnp.float32, math.log(0.01), math.log(1.0 / 30.0))
    return jnp.where(quick, fast_rate, slow_rate)


def draw_sudden_log_decay(key, part):
    where_key, depth_key = jax.random.split(key)
    struck = jax.random.randint(where_key, (TOKENS, 1), 0, TOKENS) < 4
    depth = jax.random.uniform(depth_key, (TOKENS, HEADS), jnp.float32, math.log(0.5), math.log(0.8))
    return jnp.where(struck, depth, 0.0)


def draw_stream(key, part):
    base_key, row_key = jax.random.split(key, 2)
    col_scale = 3.0 ** (jnp.arange(D, dtype=jnp.float32) / D - 0.5)
    values = jnp.clip(jax.random.normal(base_key, (TOKENS, D), jnp.float32), -6.0, 6.0)
    row_scale = jnp.exp(jax.random.uniform(row_key, (TOKENS, 1), jnp.float32, math.log(0.5), math.log(2.0)))
    return (values * row_scale * col_scale).astype(jnp.bfloat16)


def levels(stream_key, shape, cuts, low, largest):
    loudness = 1.0
    for axis_at, blocks in cuts:
        heights = jax.random.uniform(jax.random.fold_in(jax.random.fold_in(stream_key, 6), axis_at), (blocks,), jnp.float32, low / len(cuts), largest / len(cuts))
        loudness = loudness * jnp.repeat(jnp.exp(heights), shape[axis_at] // blocks).reshape((-1,) + (1,) * (len(shape) - 1 - axis_at))
    return loudness


def split_up(amount, total, bound, skew):
    weights = [(1 << 20) // math.isqrt(grade ** skew) + 1 for grade in range(2, amount + 1)]
    spare, holding = total - bound - (amount - 1), [1] * (amount - 1)
    while spare > 0:
        movable = [i for i in range(amount - 1) if holding[i] < bound]
        pool, remaining = sum([weights[i] for i in movable]), spare
        for i in movable:
            more = min(bound - holding[i], max(1, remaining * weights[i] // pool), spare)
            holding[i] = holding[i] + more
            spare = spare - more
    return np.array([bound] + holding)


def ragged_sizes(key, amount, total, reach, skew):
    if amount == 2:
        one = jax.random.randint(key, (), max(1, total - reach), min(reach, total - 1) + 1)
        return jnp.stack([one, total - one])
    sizes = jnp.asarray(split_up(amount, total, reach, skew), jnp.int32)
    twos = (amount - 1) // 2
    donor, receiver = sizes[1:1 + 2 * twos:2], sizes[2:2 + 2 * twos:2]
    margin = jnp.minimum(donor - 1, reach - receiver)
    shifted = jax.random.randint(jax.random.fold_in(key, 1), (twos,), 0, 1 << 20) % (margin + 1)
    sizes = sizes.at[1:1 + 2 * twos:2].set(donor - shifted).at[2:2 + 2 * twos:2].set(receiver + shifted)
    return sizes[jax.random.permutation(jax.random.fold_in(key, 2), amount)]


def noise(own_key, extent, deviation, most, cuts=(), kind=jnp.bfloat16):
    loudness = levels(own_key, extent, cuts, -0.22, 0.18) if cuts else 1.0
    values = jax.random.normal(own_key, extent, jnp.float32) * deviation * loudness
    return jnp.minimum(jnp.maximum(values, -most), most).astype(kind)


def setup_inputs(seed: int = 0) -> dict:
    arg_keys = jax.random.split(jax.random.key(seed), 20)
    return {
        "head_value_rows": noise(arg_keys[0], (TOKENS, INNER), 1.0, 6.0, ((0, 32), (1, 8))),
        "entry_map_rows": noise(arg_keys[1], (TOKENS, GROUPS * STATE), 1.0, 6.0, ((0, 32), (1, 8))),
        "readout_map_rows": noise(arg_keys[2], (TOKENS, GROUPS * STATE), 1.0, 6.0, ((0, 32), (1, 8))),
        "output_gate_rows": noise(arg_keys[3], (TOKENS, INNER), 1.0, 6.0, ((0, 32), (1, 8))),
        "step_before_softplus": draw_step_before_softplus(jax.random.fold_in(arg_keys[19], 71), 0),
        "sudden_log_decay": draw_sudden_log_decay(jax.random.fold_in(arg_keys[19], 71), 0),
        "document_index": jnp.searchsorted(jnp.cumsum(ragged_sizes(arg_keys[6], N_SP // 4, TOKENS, 8 * TOK_DEV, 1)), jnp.arange(TOKENS), side="right").astype(jnp.int32),
        "head_rate_logarithm": draw_head_rate_logarithm(jax.random.fold_in(arg_keys[19], 71), 0),
        "head_step_bias": noise(arg_keys[8], (2, HEADS), 0.5, 3.0, ((1, 8),), jnp.float32),
        "value_conv_taps": noise(arg_keys[9], (CONV_WIDTH, INNER), CONV_WIDTH ** -0.5, 2.5, ((1, 8),)),
        "entry_conv_taps": noise(arg_keys[10], (CONV_WIDTH, GROUPS * STATE), CONV_WIDTH ** -0.5, 2.5, ((1, 8),)),
        "readout_conv_taps": noise(arg_keys[11], (CONV_WIDTH, GROUPS * STATE), CONV_WIDTH ** -0.5, 2.5, ((1, 8),)),
        "group_norm_gain": jnp.clip(1.0 + 0.18 * jax.random.normal(arg_keys[12], (INNER,), jnp.float32), 0.1, 1.9),
        "mixer_output_weight": noise(arg_keys[13], (INNER, D), INNER ** -0.5, 0.125, ((0, 8),)),
        "stream": draw_stream(jax.random.fold_in(arg_keys[19], 71), 0),
        "mixer_norm_gain": jnp.clip(1.0 + 0.18 * jax.random.normal(arg_keys[15], (D,), jnp.float32), 0.1, 1.9),
        "channel_norm_gain": jnp.clip(1.0 + 0.18 * jax.random.normal(arg_keys[16], (D,), jnp.float32), 0.1, 1.9),
        "up_projection_weight": noise(arg_keys[17], (D, FF), D ** -0.5, 0.125, ((0, 32), (1, 8))),
        "down_projection_weight": noise(arg_keys[18], (D, FF), FF ** -0.5, 0.0625, ((0, 32), (1, 8))),
    }


exact_prec = lax.Precision.HIGHEST
norm_eps = 1e-05
resid_scale = 1.4142135623730951

def block_step(running, blocks):
    states, last_doc = running
    scaled, entries, readout, decay_logarithm, block_ids = blocks
    block_len = block_ids.shape[0]
    cum_decay = jnp.cumsum(decay_logarithm, axis=0)
    indices = lax.iota(jnp.int32, block_len)
    linked = (indices[:, None] >= indices[None, :]) & (block_ids[:, None] == block_ids[None, :])
    link_mask = linked[:, :, None, None]
    spread = cum_decay[:, None] - cum_decay[None, :]
    weights = jnp.where(link_mask, jnp.exp(jnp.where(link_mask, spread, 0.0)), 0.0)
    scores = jnp.einsum('tgn,sgn->tsg', readout, entries, precision=exact_prec)
    within = jnp.einsum('tsg,tsgr,sgrp->tgrp', scores, weights, scaled, precision=exact_prec)
    arrival = jnp.where((block_ids == last_doc)[:, None, None], jnp.exp(cum_decay), 0.0)
    carried = jnp.einsum('tgn,grpn->tgrp', readout, states, precision=exact_prec) * arrival[..., None]
    end_doc = block_ids[-1]
    to_end = jnp.where((block_ids == end_doc)[:, None, None], jnp.exp(cum_decay[-1] - cum_decay), 0.0)
    passing = jnp.where(end_doc == last_doc, jnp.exp(cum_decay[-1]), 0.0)
    fresh = jnp.einsum('sgn,sgr,sgrp->grpn', entries, to_end, scaled, precision=exact_prec)
    return ((states * passing[..., None, None] + fresh, end_doc), within + carried)

def sweep_blocks(scaled, entries, readout, decay_logarithm, document_index, states, last_doc, block_len):
    row_count = document_index.shape[0]
    block_count = row_count // block_len

    def in_blocks(array):
        return array.reshape((block_count, block_len) + array.shape[1:])
    inputs = tuple((in_blocks(array) for array in (scaled, entries, readout, decay_logarithm, document_index)))
    (states, last_doc), output = lax.scan(block_step, (states, last_doc), inputs)
    return (output.reshape((row_count,) + output.shape[2:]), states)

def short_conv(inputs, weights, document_index):
    taps = weights.shape[0]
    half_width = taps // 2
    row_count = inputs.shape[0]
    padded = jnp.pad(inputs, ((half_width, half_width), (0, 0)))
    doc_pad = jnp.pad(document_index, half_width, constant_values=-1)
    summed = jnp.zeros(inputs.shape, jnp.float32)
    for offset in range(taps):
        same_doc = (doc_pad[offset:offset + row_count] == document_index)[:, None]
        summed = summed + weights[offset] * jnp.where(same_doc, padded[offset:offset + row_count], 0.0)
    return jax.nn.silu(summed)

def layer_norm(residual, gain):
    row_mean = lax.optimization_barrier(jnp.mean(residual, axis=1))
    row_var = lax.optimization_barrier(jnp.mean(residual * residual, axis=1)) - row_mean * row_mean
    return ((residual - row_mean[:, None]) * lax.rsqrt(row_var + norm_eps)[:, None] * gain).astype(jnp.bfloat16)

def block_sums(left, right):
    parts = jnp.einsum('tjc,jcd->jtd', left, right)
    rounded = parts.astype(jnp.bfloat16)
    rounded = lax.optimization_barrier(rounded)
    return lax.optimization_barrier(jnp.sum(rounded.astype(jnp.float32), axis=0))

def reference(head_value_rows, entry_map_rows, readout_map_rows, output_gate_rows, step_before_softplus, sudden_log_decay, document_index, head_rate_logarithm, head_step_bias, value_conv_taps, entry_conv_taps, readout_conv_taps, group_norm_gain, mixer_output_weight, stream, mixer_norm_gain, channel_norm_gain, up_projection_weight, down_projection_weight):
    per_group = HEADS // GROUPS
    values = short_conv(head_value_rows.astype(jnp.float32), value_conv_taps.astype(jnp.float32), document_index)
    values = values.reshape(TOKENS, GROUPS, per_group, HEAD_DIM)
    entries = short_conv(entry_map_rows.astype(jnp.float32), entry_conv_taps.astype(jnp.float32), document_index)
    entries = entries.reshape(TOKENS, GROUPS, STATE)
    readout = short_conv(readout_map_rows.astype(jnp.float32), readout_conv_taps.astype(jnp.float32), document_index)
    readout = readout.reshape(TOKENS, GROUPS, STATE)
    summed = jnp.zeros((TOKENS, GROUPS, per_group, HEAD_DIM), jnp.float32)
    for sweep_direction in range(2):
        head_step_length = jax.nn.softplus(step_before_softplus.astype(jnp.float32) + head_step_bias[sweep_direction])
        decay_logarithm = -jnp.exp(head_rate_logarithm[sweep_direction]) * head_step_length + sudden_log_decay
        decay_logarithm = decay_logarithm.reshape(TOKENS, GROUPS, per_group)
        scaled = values * head_step_length.reshape(TOKENS, GROUPS, per_group)[..., None]
        arrays = (scaled, entries, readout, decay_logarithm, document_index)
        if sweep_direction == 1:
            arrays = tuple((jnp.flip(array, 0) for array in arrays))
        start_state = jnp.zeros((GROUPS, per_group, HEAD_DIM, STATE), jnp.float32)
        output, _ = sweep_blocks(*arrays, start_state, jnp.int32(-1), BLOCK)
        if sweep_direction == 1:
            output = jnp.flip(output, 0)
        summed = summed + output
    gated = summed.reshape(TOKENS, GROUPS, per_group * HEAD_DIM)
    gated = gated * jax.nn.silu(output_gate_rows.astype(jnp.float32)).reshape(TOKENS, GROUPS, per_group * HEAD_DIM)
    gated = gated * lax.rsqrt(lax.optimization_barrier(jnp.mean(gated * gated, axis=2, keepdims=True)) + norm_eps)
    normed = (gated.reshape(TOKENS, INNER) * group_norm_gain).astype(jnp.bfloat16)
    out_blocks = mixer_output_weight.astype(jnp.float32).reshape(N_TP, INNER // N_TP, D)
    down_blocks = down_projection_weight.astype(jnp.float32).reshape(D, N_TP, FF // N_TP)

    def dense_rows(pieces):
        normed_rows, stream_rows = pieces
        mixer_sum = block_sums(normed_rows.astype(jnp.float32).reshape(-1, N_TP, INNER // N_TP), out_blocks)
        first_sum = resid_scale * stream_rows.astype(jnp.float32) + mixer_sum
        normed_one = layer_norm(first_sum, mixer_norm_gain)
        hidden = jnp.dot(normed_one, up_projection_weight, preferred_element_type=jnp.float32)
        squared = jnp.square(jax.nn.relu(hidden)).astype(jnp.bfloat16)
        parts = jnp.einsum('tjf,djf->jtd', squared.astype(jnp.float32).reshape(-1, N_TP, FF // N_TP), down_blocks)
        rounded = lax.optimization_barrier(parts.astype(jnp.bfloat16))
        down_sum = lax.optimization_barrier(jnp.sum(rounded.astype(jnp.float32), axis=0))
        second_sum = resid_scale * normed_one.astype(jnp.float32) + down_sum
        return layer_norm(second_sum, channel_norm_gain)
    result = lax.map(dense_rows, (normed.reshape(N_SP, TOK_DEV, INNER), stream.reshape(N_SP, TOK_DEV, D)))
    return result.reshape(TOKENS, D)
```

```python
import jax
import jax.numpy as jnp
from jax import lax
from jax.experimental import pallas as pl
from jax.experimental.pallas import tpu as pltpu
from jax.sharding import Mesh
from jax.sharding import PartitionSpec as P

EPS = 1e-05
RES = 1.4142135623730951
SP = ("z", "y")
TP = ("x", "c")
ROWS = 768
HALF = 384
TILE = 256
TILES = ROWS // TILE
HI = lax.Precision.HIGHEST
F32 = jnp.float32
BF = jnp.bfloat16


def vm():
    return pl.BlockSpec(memory_space=pltpu.VMEM)


def sm():
    return pl.BlockSpec(memory_space=pltpu.SMEM)


def call(body, ins, outs, scratch=(), scalars=0, name=None, flops=0):
    return pl.pallas_call(
        body,
        in_specs=[sm()] * scalars + [vm()] * (ins - scalars),
        out_specs=[vm()] * len(outs),
        out_shape=[jax.ShapeDtypeStruct(s, d) for s, d in outs],
        scratch_shapes=list(scratch),
        name=name,
        cost_estimate=pl.CostEstimate(flops=flops, bytes_accessed=1000000, transcendentals=0),
    )


def iota(shape, dim):
    return lax.broadcasted_iota(jnp.int32, shape, dim)


def dot(a, b, ca, cb, precision=None):
    return lax.dot_general(
        a, b, (((ca,), (cb,)), ((), ())), precision=precision, preferred_element_type=F32
    )


def head_spread():
    return (iota((8, 512), 1) // 64 == iota((8, 512), 0)).astype(F32)


def conv_body(
    sp, rate, bias, v, e, r, lo, hi, tv, te, tr, step, sudden, doc,
    x_out, b_out, c_out, cum_out, dt_out, ct_out, dev_out, doc_out, si_out, pay_out, ext,
):
    base = sp[0] * 6
    rows = [doc[pl.ds(jnp.maximum(base - 1, 0), 1), :]]
    rows += [doc[pl.ds(base + k, 1), :] for k in range(6)]
    rows += [doc[pl.ds(jnp.minimum(base + 6, 191), 1), :]]
    lane = iota((1, 128), 1)
    first = jnp.where(sp[0] == 0, -1, rows[0])
    last = jnp.where(sp[0] == 31, -1, rows[7])
    window = jnp.concatenate([first] + rows[1:7] + [last], axis=1)
    own = window[:, 128:896]
    masks = []
    for d in range(-2, 3):
        moved = window if d == 0 else pltpu.roll(window, (-d) % 1024, 1)
        masks.append((moved[:, 128:896] == own).astype(F32))
    zero = jnp.zeros((1, ROWS), F32)
    mask_cols = jnp.transpose(jnp.concatenate(masks + [zero] * 3, axis=0))
    ext[8:776, 0:256] = v[...].astype(F32)
    ext[8:776, 256:384] = e[...].astype(F32)
    ext[8:776, 384:512] = r[...].astype(F32)
    ext[6:8, :] = lo[...].astype(F32)
    ext[776:778, :] = hi[...].astype(F32)
    taps = jnp.concatenate([tv[...], te[...], tr[...]], axis=1).astype(F32)
    acc = jnp.zeros((ROWS, 512), F32)
    for d in range(5):
        acc = acc + taps[d : d + 1, :] * (mask_cols[:, d : d + 1] * ext[6 + d : 6 + d + ROWS, :])
    act = acc * jax.nn.sigmoid(acc)
    x = act[:, 0:256]
    b = act[:, 256:384].astype(BF)
    x_out[...] = x.astype(BF)
    b_out[...] = b
    c_out[...] = act[:, 384:512].astype(BF)

    row = iota((8, 1), 0)
    fwd = row < 4
    rate_col = jnp.zeros((8, 1), F32)
    bias_col = jnp.zeros((8, 1), F32)
    for k in range(8):
        rate_col = jnp.where(row == k, rate[k // 4, k % 4], rate_col)
        bias_col = jnp.where(row == k, bias[k // 4, k % 4], bias_col)
    pick = (iota((8, 4), 0) % 4 == iota((8, 4), 1)).astype(F32)
    raw = dot(pick, step[...].astype(F32), 1, 1, HI) + bias_col
    dt = jnp.maximum(raw, 0.0) + jnp.log1p(jnp.exp(-jnp.abs(raw)))
    ld = -jnp.exp(rate_col) * dt + dot(pick, sudden[...], 1, 1, HI)
    dt_out[...] = dt
    dev = own.astype(F32)
    doc_out[...] = jnp.broadcast_to(dev, (8, ROWS))
    prev_id = window[:, 127:128].astype(F32)
    next_id = window[:, 896:897].astype(F32)
    upper = (iota((TILE, TILE), 0) <= iota((TILE, TILE), 1)).astype(F32)
    spread = head_spread()
    inc, exc, tot, dl, df = [], [], [], [], []
    for i in range(TILES):
        part = ld[:, i * TILE : (i + 1) * TILE]
        c = dot(part, upper, 1, 0, HI)
        inc.append(c)
        exc.append(c - part)
        tot.append(c[:, TILE - 1 : TILE])
        dl.append(dev[:, (i + 1) * TILE - 1 : (i + 1) * TILE])
        df.append(dev[:, i * TILE : i * TILE + 1])
    before = [prev_id, dl[0], dl[1]]
    after = [df[1], df[2], next_id]
    states, passing = [], []
    for i in range(TILES):
        ids = dev[:, i * TILE : (i + 1) * TILE]
        cols = slice(i * TILE, (i + 1) * TILE)
        cum_out[:, cols] = jnp.where(fwd, inc[i], exc[i])
        keep = ids == jnp.where(fwd, dl[i], df[i])
        weight = jnp.where(keep, dt[:, cols] * jnp.exp(jnp.where(fwd, tot[i] - inc[i], exc[i])), 0.0)
        wide = dot(weight, spread, 0, 0, HI)
        xi = x[i * TILE : (i + 1) * TILE, :]
        scaled = (jnp.concatenate([xi, xi], axis=1) * wide).astype(BF)
        states.append(dot(b[i * TILE : (i + 1) * TILE, :], scaled, 0, 0))
        reach = jnp.where(fwd, inc[i], tot[i] - exc[i])
        edge = jnp.where(fwd, before[i], after[i])
        ct_out[:, cols] = jnp.where(ids == edge, jnp.exp(reach), 0.0)
        far = jnp.where(fwd, sum(tot[:i], jnp.zeros((8, 1), F32)), sum(tot[i + 1 :], jnp.zeros((8, 1), F32)))
        dev_out[:, cols] = jnp.where(ids == jnp.where(fwd, prev_id, next_id), jnp.exp(reach + far), 0.0)
        through = jnp.where(jnp.where(fwd, dl[i], df[i]) == edge, jnp.exp(tot[i]), 0.0)
        passing.append(jnp.sum(through * spread, axis=0, keepdims=True))
    f = [s[:, 0:256] for s in states]
    g = [s[:, 256:512] for s in states]
    pf = [q[:, 0:256] for q in passing]
    pg = [q[:, 256:512] for q in passing]
    f2 = f[1] + pf[1] * f[0]
    g0 = g[1] + pg[1] * g[2]
    si_out[0] = f[0].astype(BF)
    si_out[1] = f2.astype(BF)
    si_out[2] = g0.astype(BF)
    si_out[3] = g[2].astype(BF)
    pay_out[0:128, 0:256] = (f[2] + pf[2] * f2).astype(BF)
    pay_out[0:128, 256:512] = (g[0] + pg[0] * g0).astype(BF)
    whole = passing[0] * passing[1] * passing[2]
    pay_out[128:144, :] = jnp.broadcast_to(whole, (16, 512)).astype(BF)


def local_body(x, b, c, cum, dt, ct, doc, si, y_out):
    spread = head_spread()
    lower = iota((TILE, TILE), 0) > iota((TILE, TILE), 1)
    upper = iota((TILE, TILE), 0) < iota((TILE, TILE), 1)
    side = iota((TILE, 128), 1) < 64
    for i in range(TILES):
        cols = slice(i * TILE, (i + 1) * TILE)
        cc = c[cols, :]
        score = dot(cc, b[cols, :], 1, 1)
        cum_row = cum[:, cols]
        cum_col = jnp.transpose(cum_row)
        ids = doc[:, cols]
        same = ids[0:1, :] == jnp.transpose(ids)[:, 0:1]
        score = jnp.where(same, score, 0.0)
        steps = dt[:, cols]
        carried = dot(ct[:, cols], spread, 0, 0, HI)
        for pair in range(2):
            xp = x[cols, pair * 128 : pair * 128 + 128]
            got = []
            for h in (2 * pair, 2 * pair + 1):
                spread_f = cum_col[:, h : h + 1] - cum_row[h : h + 1, :]
                spread_b = cum_row[h + 4 : h + 5, :] - cum_col[:, h + 4 : h + 5]
                reach = jnp.exp(jnp.where(upper, spread_b, spread_f))
                d0 = steps[h : h + 1, :]
                d1 = steps[h + 4 : h + 5, :]
                amount = jnp.where(lower, d0, jnp.where(upper, d1, d0 + d1))
                got.append(dot((score * (reach * amount)).astype(BF), xp, 1, 0))
            part = jnp.where(side, got[0], got[1])
            lanes = slice(pair * 128, pair * 128 + 128)
            wide = slice(256 + pair * 128, 384 + pair * 128)
            if i > 0:
                part = part + dot(cc, si[i - 1][:, lanes], 1, 0) * carried[:, lanes]
            if i < TILES - 1:
                part = part + dot(cc, si[i + 2][:, lanes], 1, 0) * carried[:, wide]
            y_out[cols, lanes] = part


def chain_body(where_y, pay, send_f, send_b, pre_out):
    y = where_y[0]
    for lanes, order, out in ((slice(0, 256), range(4), send_f), (slice(256, 512), range(3, -1, -1), send_b)):
        state = jnp.zeros((128, 256), F32)
        through = jnp.ones((1, 256), F32)
        pre, pre_through = state, through
        for k in order:
            pre = jnp.where(y == k, state, pre)
            pre_through = jnp.where(y == k, through, pre_through)
            hop = pay[k, 128:144, lanes].astype(F32)[0:1, :]
            state = state * hop + pay[k, 0:128, lanes].astype(F32)
            through = through * hop
        out[0:128, :] = state.astype(BF)
        out[128:144, :] = jnp.broadcast_to(through, (16, 256)).astype(BF)
        pre_out[0:128, lanes] = pre
        pre_out[128:136, lanes] = jnp.broadcast_to(pre_through, (8, 256))


def gate_body(core, yl, c, dev, pre, f1, f2, b1, b2, gate, gain, keep, send, normed):
    spread = head_spread()
    states = []
    for lanes, near, far in ((slice(0, 256), f1, f2), (slice(256, 512), b1, b2)):
        more = near[128:144, :].astype(F32)[0:1, :] * far[0:128, :].astype(F32)
        come = near[0:128, :].astype(F32) + more
        states.append((pre[0:128, lanes] + pre[128:129, lanes] * come).astype(BF))
    for i in range(TILES):
        cols = slice(i * TILE, (i + 1) * TILE)
        wide = dot(dev[:, cols], spread, 0, 0, HI)
        y = yl[cols, :]
        y = y + dot(c[cols, :], states[0], 1, 0) * wide[:, 0:256]
        y = y + dot(c[cols, :], states[1], 1, 0) * wide[:, 256:512]
        z = gate[cols, :].astype(F32)
        y = y * (z * jax.nn.sigmoid(z))
        y = y * lax.rsqrt(jnp.mean(y * y, axis=1, keepdims=True) + EPS)
        normed[cols, :] = (y * gain[...]).astype(BF)
    mine = pl.multiple_of(core[0] * HALF, HALF)
    other = pl.multiple_of(HALF - core[0] * HALF, HALF)
    keep[...] = normed[pl.ds(mine, HALF), :]
    send[...] = normed[pl.ds(other, HALF), :]


def mix_body(where_x, a, b, wa, wb, o0, o1, o2, o3):
    for k, out in ((2, o2), (1, o1), (3, o3), (0, o0)):
        block = pl.multiple_of(((where_x[0] + k) % 4) * 512, 512)
        got = dot(a[...], wa[:, pl.ds(block, 512)], 1, 0)
        got = got + dot(b[...], wb[:, pl.ds(block, 512)], 1, 0)
        out[...] = got.astype(BF)


def first_body(core, own, stream_a, stream_b, r1, r2, r3, gain_a, gain_b, out, total, gain):
    lane_a = pl.multiple_of(core[0] * 256, 256)
    lane_b = pl.multiple_of(256 - core[0] * 256, 256)
    total[:, pl.ds(lane_a, 256)] = stream_a[...].astype(F32)
    total[:, pl.ds(lane_b, 256)] = stream_b[...].astype(F32)
    gain[0:1, pl.ds(lane_a, 256)] = gain_a[0:1, :]
    gain[0:1, pl.ds(lane_b, 256)] = gain_b[0:1, :]
    mix = own[...].astype(F32) + r1[...].astype(F32) + r2[...].astype(F32) + r3[...].astype(F32)
    first = RES * total[...] + mix
    mean = jnp.mean(first, axis=1, keepdims=True).astype(BF).astype(F32)
    out[0:HALF, :] = (first - mean).astype(BF)
    means = jnp.transpose(jnp.broadcast_to(mean, (HALF, 128)))[0:1, :]
    means = jnp.concatenate([means, jnp.zeros((1, 128), F32)], axis=1)
    g = gain[0:1, :]
    g0 = g.astype(BF).astype(F32)
    g1 = (g - g0).astype(BF).astype(F32)
    g2 = g - g0 - g1
    row = iota((16, 512), 0)
    tail = jnp.where(row == 0, means, jnp.where(row == 1, g0, jnp.where(row == 2, g1, jnp.where(row == 3, g2, 0.0))))
    out[HALF : HALF + 16, :] = tail.astype(BF)


def up_body(where_x, p0, p1, p2, p3, w, hidden, resid, xn):
    @pl.when(pl.program_id(0) == 0)
    def _():
        blocks = (p0, p1, p2, p3)
        tails = [p[HALF : HALF + 16, :].astype(F32) for p in blocks]
        means = jnp.concatenate([t[0:1, 0:HALF] for t in tails] + [jnp.zeros((4, HALF), F32)], axis=0)
        mean_cols = jnp.transpose(means)
        full = [p[0:HALF, :].astype(F32) + mean_cols[:, k : k + 1] for k, p in enumerate(blocks)]
        m = sum(jnp.sum(q, axis=1, keepdims=True) for q in full) / 2048.0
        full = [q - m for q in full]
        v = sum(jnp.sum(q * q, axis=1, keepdims=True) for q in full) / 2048.0
        scale = lax.rsqrt(v + EPS)
        for k, q in enumerate(full):
            gain = tails[k][1:2, :] + tails[k][2:3, :] + tails[k][3:4, :]
            done = (q * scale * gain).astype(BF)
            block = pl.multiple_of(((where_x[0] + (4 - k)) % 4) * 512, 512)
            xn[:, pl.ds(block, 512)] = done
            if k == 0:
                resid[...] = done

    got = dot(xn[...], w[...].reshape(2048, 512), 1, 0)
    got = jnp.maximum(got, 0.0)
    hidden[...] = (got * got).astype(BF)


def down_body(where_x, h, w, out, acc):
    got = dot(h[...], w[...].reshape(512, 1024), 1, 1)

    @pl.when(pl.program_id(0) == 0)
    def _():
        acc[...] = got

    @pl.when(pl.program_id(0) == 1)
    def _():
        out[...] = (acc[...] + got).astype(BF)


def second_body(resid, own, r1, r2, r3, second, stats):
    total = own[...].astype(F32) + r1[...].astype(F32) + r2[...].astype(F32) + r3[...].astype(F32)
    total = RES * resid[...].astype(F32) + total
    second[...] = total
    s1 = jnp.transpose(jnp.broadcast_to(jnp.sum(total, axis=1, keepdims=True), (HALF, 128)))[0:8, :]
    s2 = jnp.transpose(jnp.broadcast_to(jnp.sum(total * total, axis=1, keepdims=True), (HALF, 128)))[0:8, :]
    stats[...] = jnp.where(iota((8, HALF), 0) == 0, s1, s2)


def last_body(core, second, s0, s1, s2, s3, gain_a, gain_b, keep, send):
    stats = s0[...] + s1[...] + s2[...] + s3[...]
    cols = jnp.transpose(stats)
    m = cols[:, 0:1] / 2048.0
    v = cols[:, 1:2] / 2048.0 - m * m
    scale = lax.rsqrt(v + EPS)
    for off, gain, out in ((core[0], gain_a, keep), (1 - core[0], gain_b, send)):
        lanes = pl.multiple_of(off * 256, 256)
        out[...] = ((second[:, pl.ds(lanes, 256)] - m) * scale * gain[1:2, :]).astype(BF)


def per_device(
    head_value_rows,
    entry_map_rows,
    readout_map_rows,
    output_gate_rows,
    step_before_softplus,
    sudden_log_decay,
    document_index,
    head_rate_logarithm,
    head_step_bias,
    value_conv_taps,
    entry_conv_taps,
    readout_conv_taps,
    group_norm_gain,
    mixer_output_weight,
    stream,
    mixer_norm_gain,
    channel_norm_gain,
    up_projection_weight,
    down_projection_weight,
):
    core = lax.axis_index("c")
    at_x = jnp.reshape(lax.axis_index("x"), (1,))
    at_c = jnp.reshape(core, (1,))
    at_y = jnp.reshape(lax.axis_index("y"), (1,))
    at_sp = jnp.reshape(lax.axis_index(SP), (1,))
    swap = [(0, 1), (1, 0)]

    def shift(a, axis, by, count):
        return lax.ppermute(a, axis, [(i, i + by) for i in range(count) if 0 <= i + by < count])

    def around(a, by):
        return lax.ppermute(a, "x", [(i, (i + by) % 4) for i in range(4)])

    tail = jnp.concatenate([a[ROWS - 2 :] for a in (head_value_rows, entry_map_rows, readout_map_rows)], axis=1)
    head = jnp.concatenate([a[:2] for a in (head_value_rows, entry_map_rows, readout_map_rows)], axis=1)
    low = shift(tail, SP, 1, 32)
    high = shift(head, SP, -1, 32)

    weights = jnp.concatenate([up_projection_weight, down_projection_weight], axis=1)
    weights = lax.all_gather(weights, ("z", "y", "c"), axis=0, tiled=True).reshape(32, 2, 64, 2048)

    weight_other = lax.ppermute(mixer_output_weight, "c", swap)
    stream_mine = lax.dynamic_slice_in_dim(stream, core * HALF, HALF)
    stream_other = lax.ppermute(lax.dynamic_slice_in_dim(stream, (1 - core) * HALF, HALF), "c", swap)
    gains = jnp.stack([mixer_norm_gain, channel_norm_gain])
    gains_other = lax.ppermute(gains, "c", swap)

    x, b, c, cum, dt, ct, dev, doc, si, pay = call(
        conv_body,
        14,
        [((ROWS, 256), BF), ((ROWS, 128), BF), ((ROWS, 128), BF)]
        + [((8, ROWS), F32)] * 5
        + [((4, 128, 256), BF), ((144, 512), BF)],
        scratch=[pltpu.VMEM((784, 512), F32)],
        scalars=3,
        name="conv_states",
        flops=10**9,
    )(
        at_sp, head_rate_logarithm, head_step_bias, head_value_rows, entry_map_rows, readout_map_rows,
        low, high, value_conv_taps, entry_conv_taps, readout_conv_taps, step_before_softplus,
        sudden_log_decay, document_index.reshape(192, 128),
    )
    rows = lax.all_gather(pay, "y")
    send_f, send_b, pre = call(
        chain_body, 2, [((144, 256), BF), ((144, 256), BF), ((136, 512), F32)], scalars=1, name="chain", flops=10**8
    )(at_y, rows)
    f1, f2 = shift(send_f, "z", 1, 8), shift(send_f, "z", 2, 8)
    b1, b2 = shift(send_b, "z", -1, 8), shift(send_b, "z", -2, 8)
    yl = call(local_body, 8, [((ROWS, 256), F32)], name="local", flops=2 * 10**9)(x, b, c, cum, dt, ct, doc, si)[0]
    keep, send = call(
        gate_body, 11, [((HALF, 256), BF)] * 2, scratch=[pltpu.VMEM((ROWS, 256), BF)], scalars=1, name="gate", flops=10**9
    )(at_c, yl, c, dev, pre, f1, f2, b1, b2, output_gate_rows, group_norm_gain.reshape(1, 256))
    other = lax.ppermute(send, "c", swap)
    o0, o1, o2, o3 = call(mix_body, 5, [((HALF, 512), BF)] * 4, scalars=1, name="mix", flops=10**9)(
        at_x, keep, other, mixer_output_weight, weight_other
    )
    r2, r1, r3 = around(o2, 2), around(o1, 1), around(o3, 3)
    p0 = call(
        first_body,
        9,
        [((HALF + 16, 512), BF)],
        scratch=[pltpu.VMEM((HALF, 512), F32), pltpu.VMEM((8, 512), F32)],
        scalars=1,
        name="first",
        flops=10**8,
    )(at_c, o0, stream_mine, stream_other, r1, r2, r3, gains, gains_other)[0]
    p2, p1, p3 = around(p0, 2), around(p0, 1), around(p0, 3)
    fixed = pl.BlockSpec((HALF + 16, 512), lambda s, _: (0, 0))
    hidden, resid = pl.pallas_call(
        up_body,
        grid_spec=pltpu.PrefetchScalarGridSpec(
            num_scalar_prefetch=1,
            grid=(4,),
            in_specs=[fixed] * 4 + [pl.BlockSpec((32, 1, 64, 512), lambda s, _: (0, s // 2, 0, s % 2))],
            out_specs=[
                pl.BlockSpec((HALF, 512), lambda s, _: (0, s)),
                pl.BlockSpec((HALF, 512), lambda s, _: (0, 0)),
            ],
            scratch_shapes=[pltpu.VMEM((HALF, 2048), BF)],
        ),
        out_shape=[jax.ShapeDtypeStruct((HALF, 2048), BF), jax.ShapeDtypeStruct((HALF, 512), BF)],
        name="up",
        cost_estimate=pl.CostEstimate(flops=3 * 10**9, bytes_accessed=10**7, transcendentals=0),
    )(at_x, p0, p1, p2, p3, weights)

    def down(k):
        return pl.pallas_call(
            down_body,
            grid_spec=pltpu.PrefetchScalarGridSpec(
                num_scalar_prefetch=1,
                grid=(2,),
                in_specs=[
                    pl.BlockSpec((HALF, 1024), lambda s, _: (0, s)),
                    pl.BlockSpec((8, 1, 64, 1024), lambda s, at: ((at[0] + k) % 4, s, 0, 1)),
                ],
                out_specs=pl.BlockSpec((HALF, 512), lambda s, _: (0, 0)),
                scratch_shapes=[pltpu.VMEM((HALF, 512), F32)],
            ),
            out_shape=jax.ShapeDtypeStruct((HALF, 512), BF),
            name="down",
            cost_estimate=pl.CostEstimate(flops=8 * 10**8, bytes_accessed=3 * 10**6, transcendentals=0),
        )(at_x, hidden, weights)

    d2, d1, d3, d0 = down(2), down(1), down(3), down(0)
    q2, q1, q3 = around(d2, 2), around(d1, 1), around(d3, 3)
    second, stats = call(second_body, 5, [((HALF, 512), F32), ((8, HALF), F32)], name="second", flops=10**8)(
        resid, d0, q1, q2, q3
    )
    s1, s2, s3 = around(stats, 1), around(stats, 2), around(stats, 3)
    keep, send = call(last_body, 8, [((HALF, 256), BF)] * 2, scalars=1, name="last", flops=10**8)(
        at_c, second, stats, s1, s2, s3, gains, gains_other
    )
    got = lax.ppermute(send, "c", swap)
    lower = core == 0
    return jnp.concatenate([jnp.where(lower, keep, got), jnp.where(lower, got, keep)], axis=0)


def solution(mesh):
    torus = Mesh(mesh.devices.reshape(8, 4, 4, 2), ("z", "y", "x", "c"))
    return jax.shard_map(
        per_device,
        mesh=torus,
        in_specs=(
            P(SP, TP),
            P(SP, TP),
            P(SP, TP),
            P(SP, TP),
            P(SP, TP),
            P(SP, TP),
            P(),
            P(None, TP),
            P(None, TP),
            P(None, TP),
            P(None, TP),
            P(None, TP),
            P(TP),
            P(TP, None),
            P(SP, TP),
            P(TP),
            P(TP),
            P(SP, TP),
            P(SP, TP),
        ),
        out_specs=P(SP, TP),
        check_vma=False,
    )
```

```python
from functools import partial

import jax
import jax.numpy as jnp
from jax import lax
from jax.experimental import pallas as pl
from jax.experimental.pallas import tpu as pltpu
from jax.sharding import Mesh
from jax.sharding import PartitionSpec as P

EPS = 1e-05
RES = 1.4142135623730951
SP = ("z", "y")
TP = ("x", "c")
ROWS = 768
HALF = 384
TILE = 256
TILES = ROWS // TILE
HI = lax.Precision.HIGHEST
F32 = jnp.float32
BF = jnp.bfloat16


def vm():
    return pl.BlockSpec(memory_space=pltpu.VMEM)


def sm():
    return pl.BlockSpec(memory_space=pltpu.SMEM)


def near(a):
    return pltpu.with_memory_space_constraint(a, pltpu.VMEM)


def off(a):
    return pltpu.with_memory_space_constraint(a, pltpu.HBM)


def call(body, ins, outs, scratch=(), scalars=0, far=(), plain=()):
    run = pl.pallas_call(
        body,
        in_specs=[sm()] * scalars + [vm()] * (ins - scalars),
        out_specs=[vm()] * len(outs),
        out_shape=[(jax.ShapeDtypeStruct if k in plain else pltpu.VMEM)(*o) for k, o in enumerate(outs)],
        scratch_shapes=list(scratch),
        compiler_params=pltpu.CompilerParams(vmem_limit_bytes=24 * 2**20),
    )
    return lambda *a: run(*[off(b) if k in far else b if k < scalars else near(b) for k, b in enumerate(a)])


def iota(shape, dim):
    return lax.broadcasted_iota(jnp.int32, shape, dim)


def dot(a, b, ca, cb, precision=None):
    return lax.dot_general(
        a, b, (((ca,), (cb,)), ((), ())), precision=precision, preferred_element_type=F32
    )


def head_spread():
    return (iota((8, 512), 1) // 64 == iota((8, 512), 0)).astype(F32)


def conv_body(
    sp, rate, bias, v, e, r, lo, hi, tv, te, tr, step, sudden, doc,
    x_out, b_out, c_out, cum_out, dt_out, ct_out, dev_out, doc_out, si_out, pay_out, ext,
):
    base = sp[0] * 6
    rows = [doc[pl.ds(jnp.maximum(base - 1, 0), 1), :]]
    rows += [doc[pl.ds(base + k, 1), :] for k in range(6)]
    rows += [doc[pl.ds(jnp.minimum(base + 6, 191), 1), :]]
    lane = iota((1, 128), 1)
    first = jnp.where(sp[0] == 0, -1, rows[0])
    last = jnp.where(sp[0] == 31, -1, rows[7])
    window = jnp.concatenate([first] + rows[1:7] + [last], axis=1)
    own = window[:, 128:896]
    masks = []
    for d in range(-2, 3):
        moved = window if d == 0 else pltpu.roll(window, (-d) % 1024, 1)
        masks.append((moved[:, 128:896] == own).astype(F32))
    zero = jnp.zeros((1, ROWS), F32)
    mask_cols = jnp.transpose(jnp.concatenate(masks + [zero] * 3, axis=0))
    ext[8:776, 0:256] = v[...].astype(F32)
    ext[8:776, 256:384] = e[...].astype(F32)
    ext[8:776, 384:512] = r[...].astype(F32)
    ext[6:8, :] = lo[...].astype(F32)
    ext[776:778, :] = hi[...].astype(F32)
    taps = jnp.concatenate([tv[...], te[...], tr[...]], axis=1).astype(F32)
    acc = jnp.zeros((ROWS, 512), F32)
    for d in range(5):
        acc = acc + taps[d : d + 1, :] * (mask_cols[:, d : d + 1] * ext[6 + d : 6 + d + ROWS, :])
    act = acc * jax.nn.sigmoid(acc)
    x = act[:, 0:256]
    b = act[:, 256:384].astype(BF)
    x_out[...] = x.astype(BF)
    b_out[...] = b
    c_out[...] = act[:, 384:512].astype(BF)

    row = iota((8, 1), 0)
    fwd = row < 4
    rate_col = jnp.zeros((8, 1), F32)
    bias_col = jnp.zeros((8, 1), F32)
    for k in range(8):
        rate_col = jnp.where(row == k, rate[k // 4, k % 4], rate_col)
        bias_col = jnp.where(row == k, bias[k // 4, k % 4], bias_col)
    pick = (iota((8, 4), 0) % 4 == iota((8, 4), 1)).astype(F32)
    raw = dot(pick, step[...].astype(F32), 1, 1, HI) + bias_col
    dt = jnp.maximum(raw, 0.0) + jnp.log1p(jnp.exp(-jnp.abs(raw)))
    ld = -jnp.exp(rate_col) * dt + dot(pick, sudden[...], 1, 1, HI)
    dt_out[...] = dt
    dev = own.astype(F32)
    doc_out[...] = jnp.broadcast_to(dev, (8, ROWS))
    prev_id = window[:, 127:128].astype(F32)
    next_id = window[:, 896:897].astype(F32)
    upper = (iota((TILE, TILE), 0) <= iota((TILE, TILE), 1)).astype(F32)
    spread = head_spread()
    inc, exc, tot, dl, df = [], [], [], [], []
    for i in range(TILES):
        part = ld[:, i * TILE : (i + 1) * TILE]
        c = dot(part, upper, 1, 0, HI)
        inc.append(c)
        exc.append(c - part)
        tot.append(c[:, TILE - 1 : TILE])
        dl.append(dev[:, (i + 1) * TILE - 1 : (i + 1) * TILE])
        df.append(dev[:, i * TILE : i * TILE + 1])
    before = [prev_id, dl[0], dl[1]]
    after = [df[1], df[2], next_id]
    states, passing = [], []
    for i in range(TILES):
        ids = dev[:, i * TILE : (i + 1) * TILE]
        cols = slice(i * TILE, (i + 1) * TILE)
        cum_out[:, cols] = jnp.where(fwd, inc[i], exc[i])
        keep = ids == jnp.where(fwd, dl[i], df[i])
        weight = jnp.where(keep, dt[:, cols] * jnp.exp(jnp.where(fwd, tot[i] - inc[i], exc[i])), 0.0)
        wide = dot(weight, spread, 0, 0, HI)
        xi = x[i * TILE : (i + 1) * TILE, :]
        scaled = (jnp.concatenate([xi, xi], axis=1) * wide).astype(BF)
        states.append(dot(b[i * TILE : (i + 1) * TILE, :], scaled, 0, 0))
        reach = jnp.where(fwd, inc[i], tot[i] - exc[i])
        edge = jnp.where(fwd, before[i], after[i])
        ct_out[:, cols] = jnp.where(ids == edge, jnp.exp(reach), 0.0)
        far = jnp.where(fwd, sum(tot[:i], jnp.zeros((8, 1), F32)), sum(tot[i + 1 :], jnp.zeros((8, 1), F32)))
        dev_out[:, cols] = jnp.where(ids == jnp.where(fwd, prev_id, next_id), jnp.exp(reach + far), 0.0)
        through = jnp.where(jnp.where(fwd, dl[i], df[i]) == edge, jnp.exp(tot[i]), 0.0)
        passing.append(jnp.sum(through * spread, axis=0, keepdims=True))
    f = [s[:, 0:256] for s in states]
    g = [s[:, 256:512] for s in states]
    pf = [q[:, 0:256] for q in passing]
    pg = [q[:, 256:512] for q in passing]
    f2 = f[1] + pf[1] * f[0]
    g0 = g[1] + pg[1] * g[2]
    si_out[0] = f[0].astype(BF)
    si_out[1] = f2.astype(BF)
    si_out[2] = g0.astype(BF)
    si_out[3] = g[2].astype(BF)
    pay_out[0:128, 0:256] = (f[2] + pf[2] * f2).astype(BF)
    pay_out[0:128, 256:512] = (g[0] + pg[0] * g0).astype(BF)
    whole = passing[0] * passing[1] * passing[2]
    pay_out[128:144, :] = jnp.broadcast_to(whole, (16, 512)).astype(BF)


def local_body(x, b, c, cum, dt, ct, doc, si, y_out):
    spread = head_spread()
    lower = iota((TILE, TILE), 0) > iota((TILE, TILE), 1)
    upper = iota((TILE, TILE), 0) < iota((TILE, TILE), 1)
    side = iota((TILE, 128), 1) < 64
    for i in range(TILES):
        cols = slice(i * TILE, (i + 1) * TILE)
        cc = c[cols, :]
        score = dot(cc, b[cols, :], 1, 1)
        cum_row = cum[:, cols]
        cum_col = jnp.transpose(cum_row)
        ids = doc[:, cols]
        same = ids[0:1, :] == jnp.transpose(ids)[:, 0:1]
        score = jnp.where(same, score, 0.0)
        steps = dt[:, cols]
        carried = dot(ct[:, cols], spread, 0, 0, HI)
        for pair in range(2):
            xp = x[cols, pair * 128 : pair * 128 + 128]
            got = []
            for h in (2 * pair, 2 * pair + 1):
                spread_f = cum_col[:, h : h + 1] - cum_row[h : h + 1, :]
                spread_b = cum_row[h + 4 : h + 5, :] - cum_col[:, h + 4 : h + 5]
                reach = jnp.exp(jnp.where(upper, spread_b, spread_f))
                d0 = steps[h : h + 1, :]
                d1 = steps[h + 4 : h + 5, :]
                amount = jnp.where(lower, d0, jnp.where(upper, d1, d0 + d1))
                got.append(dot((score * (reach * amount)).astype(BF), xp, 1, 0))
            part = jnp.where(side, got[0], got[1])
            lanes = slice(pair * 128, pair * 128 + 128)
            wide = slice(256 + pair * 128, 384 + pair * 128)
            if i > 0:
                part = part + dot(cc, si[i - 1][:, lanes], 1, 0) * carried[:, lanes]
            if i < TILES - 1:
                part = part + dot(cc, si[i + 2][:, lanes], 1, 0) * carried[:, wide]
            y_out[cols, lanes] = part


def chain_body(where_y, pay, send_f, send_b, pre_out):
    y = where_y[0]
    for lanes, order, out in ((slice(0, 256), range(4), send_f), (slice(256, 512), range(3, -1, -1), send_b)):
        state = jnp.zeros((128, 256), F32)
        through = jnp.ones((1, 256), F32)
        pre, pre_through = state, through
        for k in order:
            pre = jnp.where(y == k, state, pre)
            pre_through = jnp.where(y == k, through, pre_through)
            hop = pay[k, 128:144, lanes].astype(F32)[0:1, :]
            state = state * hop + pay[k, 0:128, lanes].astype(F32)
            through = through * hop
        out[0:128, :] = state.astype(BF)
        out[128:144, :] = jnp.broadcast_to(through, (16, 256)).astype(BF)
        pre_out[0:128, lanes] = pre
        pre_out[128:136, lanes] = jnp.broadcast_to(pre_through, (8, 256))


def gate_body(core, yl, c, dev, pre, f1, f2, b1, b2, gate, gain, keep, send, normed):
    spread = head_spread()
    states = []
    for lanes, near, far in ((slice(0, 256), f1, f2), (slice(256, 512), b1, b2)):
        more = near[128:144, :].astype(F32)[0:1, :] * far[0:128, :].astype(F32)
        come = near[0:128, :].astype(F32) + more
        states.append((pre[0:128, lanes] + pre[128:129, lanes] * come).astype(BF))
    for i in range(TILES):
        cols = slice(i * TILE, (i + 1) * TILE)
        wide = dot(dev[:, cols], spread, 0, 0, HI)
        y = yl[cols, :]
        y = y + dot(c[cols, :], states[0], 1, 0) * wide[:, 0:256]
        y = y + dot(c[cols, :], states[1], 1, 0) * wide[:, 256:512]
        z = gate[cols, :].astype(F32)
        y = y * (z * jax.nn.sigmoid(z))
        y = y * lax.rsqrt(jnp.mean(y * y, axis=1, keepdims=True) + EPS)
        normed[cols, :] = (y * gain[...]).astype(BF)
    mine = pl.multiple_of(core[0] * HALF, HALF)
    other = pl.multiple_of(HALF - core[0] * HALF, HALF)
    keep[...] = normed[pl.ds(mine, HALF), :]
    send[...] = normed[pl.ds(other, HALF), :]


def mix_body(where_x, a, b, wa, wb, o0, o1, o2, o3):
    for k, out in ((2, o2), (1, o1), (3, o3), (0, o0)):
        block = pl.multiple_of(((where_x[0] + k) % 4) * 512, 512)
        got = dot(a[...], wa[:, pl.ds(block, 512)], 1, 0)
        got = got + dot(b[...], wb[:, pl.ds(block, 512)], 1, 0)
        out[...] = got.astype(BF)


def first_body(core, own, stream_a, stream_b, r1, r2, r3, gain_a, gain_b, out, total, gain):
    lane_a = pl.multiple_of(core[0] * 256, 256)
    lane_b = pl.multiple_of(256 - core[0] * 256, 256)
    total[:, pl.ds(lane_a, 256)] = stream_a[...].astype(F32)
    total[:, pl.ds(lane_b, 256)] = stream_b[...].astype(F32)
    gain[0:1, pl.ds(lane_a, 256)] = gain_a[0:1, :]
    gain[0:1, pl.ds(lane_b, 256)] = gain_b[0:1, :]
    mix = own[...].astype(F32) + r1[...].astype(F32) + r2[...].astype(F32) + r3[...].astype(F32)
    first = RES * total[...] + mix
    mean = jnp.mean(first, axis=1, keepdims=True).astype(BF).astype(F32)
    out[0:HALF, :] = (first - mean).astype(BF)
    means = jnp.transpose(jnp.broadcast_to(mean, (HALF, 128)))[0:1, :]
    means = jnp.concatenate([means, jnp.zeros((1, 128), F32)], axis=1)
    g = gain[0:1, :]
    g0 = g.astype(BF).astype(F32)
    g1 = (g - g0).astype(BF).astype(F32)
    g2 = g - g0 - g1
    row = iota((16, 512), 0)
    tail = jnp.where(row == 0, means, jnp.where(row == 1, g0, jnp.where(row == 2, g1, jnp.where(row == 3, g2, 0.0))))
    out[HALF : HALF + 16, :] = tail.astype(BF)


def up_body(where_x, p0, p1, p2, p3, w, hidden, resid, down, xn, up, sems):
    loads = []
    for core in range(2):
        for part in range(2):
            lanes = slice(part * 512, part * 512 + 512)
            loads.append((w.at[:, core, :, lanes], up.at[2 * core + part]))
    for block in range(4):
        rows = slice(block * 8, block * 8 + 8)
        loads.append((w.at[rows, :, :, 1024:2048], down.at[rows]))
    loads = [pltpu.make_async_copy(src, dst, sems.at[k]) for k, (src, dst) in enumerate(loads)]
    for load in loads:
        load.start()
    blocks = (p0, p1, p2, p3)
    tails = [p[HALF : HALF + 16, :].astype(F32) for p in blocks]
    means = jnp.concatenate([t[0:1, 0:HALF] for t in tails] + [jnp.zeros((4, HALF), F32)], axis=0)
    mean_cols = jnp.transpose(means)
    full = [p[0:HALF, :].astype(F32) + mean_cols[:, k : k + 1] for k, p in enumerate(blocks)]
    m = sum(jnp.sum(q, axis=1, keepdims=True) for q in full) / 2048.0
    full = [q - m for q in full]
    v = sum(jnp.sum(q * q, axis=1, keepdims=True) for q in full) / 2048.0
    scale = lax.rsqrt(v + EPS)
    for k, q in enumerate(full):
        gain = tails[k][1:2, :] + tails[k][2:3, :] + tails[k][3:4, :]
        done = (q * scale * gain).astype(BF)
        block = pl.multiple_of(((where_x[0] + (4 - k)) % 4) * 512, 512)
        xn[:, pl.ds(block, 512)] = done
        if k == 0:
            resid[...] = done
    for k in range(4):
        loads[k].wait()
        got = jnp.maximum(dot(xn[...], up[k].reshape(2048, 512), 1, 0), 0.0)
        hidden[:, k * 512 : k * 512 + 512] = (got * got).astype(BF)
    for k in range(4, 8):
        loads[k].wait()


def down_body(block, where_x, h, w, out):
    rows = pl.ds(((where_x[0] + block) % 4) * 8, 8)
    got = dot(h[:, 0:1024], w[rows, 0].reshape(512, 1024), 1, 1)
    out[...] = (got + dot(h[:, 1024:2048], w[rows, 1].reshape(512, 1024), 1, 1)).astype(BF)


def second_body(resid, own, r1, r2, r3, second, stats):
    total = own[...].astype(F32) + r1[...].astype(F32) + r2[...].astype(F32) + r3[...].astype(F32)
    total = RES * resid[...].astype(F32) + total
    second[...] = total
    s1 = jnp.transpose(jnp.broadcast_to(jnp.sum(total, axis=1, keepdims=True), (HALF, 128)))[0:8, :]
    s2 = jnp.transpose(jnp.broadcast_to(jnp.sum(total * total, axis=1, keepdims=True), (HALF, 128)))[0:8, :]
    stats[...] = jnp.where(iota((8, HALF), 0) == 0, s1, s2)


def last_body(core, second, s0, s1, s2, s3, gain_a, gain_b, full, send):
    stats = s0[...] + s1[...] + s2[...] + s3[...]
    cols = jnp.transpose(stats)
    m = cols[:, 0:1] / 2048.0
    v = cols[:, 1:2] / 2048.0 - m * m
    scale = lax.rsqrt(v + EPS)
    mine = pl.multiple_of(core[0] * 256, 256)
    other = pl.multiple_of(256 - core[0] * 256, 256)
    send[...] = ((second[:, pl.ds(other, 256)] - m) * scale * gain_b[1:2, :]).astype(BF)
    rows = pl.ds(pl.multiple_of(core[0] * HALF, HALF), HALF)
    full[rows, :] = ((second[:, pl.ds(mine, 256)] - m) * scale * gain_a[1:2, :]).astype(BF)


def layer(
    head_value_rows,
    entry_map_rows,
    readout_map_rows,
    output_gate_rows,
    step_before_softplus,
    sudden_log_decay,
    document_index,
    head_rate_logarithm,
    head_step_bias,
    value_conv_taps,
    entry_conv_taps,
    readout_conv_taps,
    group_norm_gain,
    mixer_output_weight,
    stream,
    mixer_norm_gain,
    channel_norm_gain,
    up_projection_weight,
    down_projection_weight,
):
    core = lax.axis_index("c")
    at_x = jnp.reshape(lax.axis_index("x"), (1,))
    at_c = jnp.reshape(core, (1,))
    at_y = jnp.reshape(lax.axis_index("y"), (1,))
    at_sp = jnp.reshape(lax.axis_index(SP), (1,))
    swap = [(0, 1), (1, 0)]

    def shift(a, axis, by, count):
        return lax.ppermute(a, axis, [(i, i + by) for i in range(count) if 0 <= i + by < count])

    def around(a, by):
        return lax.ppermute(a, "x", [(i, (i + by) % 4) for i in range(4)])

    tail = jnp.concatenate([a[ROWS - 2 :] for a in (head_value_rows, entry_map_rows, readout_map_rows)], axis=1)
    head = jnp.concatenate([a[:2] for a in (head_value_rows, entry_map_rows, readout_map_rows)], axis=1)
    low = shift(tail, SP, 1, 32)
    high = shift(head, SP, -1, 32)

    weights = jnp.concatenate([up_projection_weight, down_projection_weight], axis=1)
    weights = lax.all_gather(weights, ("z", "y", "c"), axis=0, tiled=True).reshape(32, 2, 64, 2048)

    weight_other = lax.ppermute(mixer_output_weight, "c", swap)
    stream_mine = lax.dynamic_slice_in_dim(stream, core * HALF, HALF)
    stream_other = lax.ppermute(lax.dynamic_slice_in_dim(stream, (1 - core) * HALF, HALF), "c", swap)
    gains = jnp.stack([mixer_norm_gain, channel_norm_gain])
    gains_other = lax.ppermute(gains, "c", swap)

    x, b, c, cum, dt, ct, dev, doc, si, pay = call(
        conv_body,
        14,
        [((ROWS, 256), BF), ((ROWS, 128), BF), ((ROWS, 128), BF)]
        + [((8, ROWS), F32)] * 5
        + [((4, 128, 256), BF), ((144, 512), BF)],
        scratch=[pltpu.VMEM((784, 512), F32)],
        scalars=3,
        far=(1, 2, 3, 4, 5, 8, 9, 10, 13),
    )(
        at_sp, head_rate_logarithm, head_step_bias, head_value_rows, entry_map_rows, readout_map_rows,
        low, high, value_conv_taps, entry_conv_taps, readout_conv_taps, step_before_softplus,
        sudden_log_decay, document_index.reshape(192, 128),
    )
    rows = lax.all_gather(pay, "y")
    send_f, send_b, pre = call(
        chain_body, 2, [((144, 256), BF), ((144, 256), BF), ((136, 512), F32)], scalars=1
    )(at_y, rows)
    f1, f2 = shift(send_f, "z", 1, 8), shift(send_f, "z", 2, 8)
    b1, b2 = shift(send_b, "z", -1, 8), shift(send_b, "z", -2, 8)
    yl = call(local_body, 8, [((ROWS, 256), F32)])(x, b, c, cum, dt, ct, doc, si)[0]
    keep, send = call(
        gate_body, 11, [((HALF, 256), BF)] * 2, scratch=[pltpu.VMEM((ROWS, 256), BF)], scalars=1, far=(9, 10)
    )(at_c, yl, c, dev, pre, f1, f2, b1, b2, output_gate_rows, group_norm_gain.reshape(1, 256))
    other = lax.ppermute(send, "c", swap)
    o0, o1, o2, o3 = call(mix_body, 5, [((HALF, 512), BF)] * 4, scalars=1, far=(3,))(
        at_x, keep, other, mixer_output_weight, weight_other
    )
    r2, r1, r3 = around(o2, 2), around(o1, 1), around(o3, 3)
    p0 = call(
        first_body,
        9,
        [((HALF + 16, 512), BF)],
        scratch=[pltpu.VMEM((HALF, 512), F32), pltpu.VMEM((8, 512), F32)],
        scalars=1,
    )(at_c, o0, stream_mine, stream_other, r1, r2, r3, gains, gains_other)[0]
    p2, p1, p3 = around(p0, 2), around(p0, 1), around(p0, 3)
    hidden, resid, down_weights = pl.pallas_call(
        up_body,
        in_specs=[sm()] + [vm()] * 4 + [pl.BlockSpec(memory_space=pltpu.HBM)],
        out_specs=[vm()] * 3,
        out_shape=[
            pltpu.VMEM((HALF, 2048), BF),
            pltpu.VMEM((HALF, 512), BF),
            pltpu.VMEM((32, 2, 64, 1024), BF),
        ],
        scratch_shapes=[
            pltpu.VMEM((HALF, 2048), BF),
            pltpu.VMEM((4, 32, 64, 512), BF),
            pltpu.SemaphoreType.DMA((8,)),
        ],
        compiler_params=pltpu.CompilerParams(vmem_limit_bytes=32 * 2**20),
        name="up",
    )(at_x, near(p0), near(p1), near(p2), near(p3), off(weights))

    def down(k):
        return call(partial(down_body, k), 3, [((HALF, 512), BF)], scalars=1)(at_x, hidden, down_weights)[0]

    d2, d1, d3, d0 = down(2), down(1), down(3), down(0)
    q2, q1, q3 = around(d2, 2), around(d1, 1), around(d3, 3)
    second, stats = call(second_body, 5, [((HALF, 512), F32), ((8, HALF), F32)])(
        resid, d0, q1, q2, q3
    )
    s1, s2, s3 = around(stats, 1), around(stats, 2), around(stats, 3)
    full, send = call(last_body, 8, [((ROWS, 256), BF), ((HALF, 256), BF)], scalars=1, plain=(0,))(
        at_c, second, stats, s1, s2, s3, gains, gains_other
    )
    got = lax.ppermute(send, "c", swap)
    return lax.dynamic_update_slice_in_dim(full, got, (1 - core) * HALF, 0)


def solution(mesh):
    torus = Mesh(mesh.devices.reshape(8, 4, 4, 2), ("z", "y", "x", "c"))
    return jax.shard_map(
        layer,
        mesh=torus,
        in_specs=(
            P(SP, TP),
            P(SP, TP),
            P(SP, TP),
            P(SP, TP),
            P(SP, TP),
            P(SP, TP),
            P(),
            P(None, TP),
            P(None, TP),
            P(None, TP),
            P(None, TP),
            P(None, TP),
            P(TP),
            P(TP, None),
            P(SP, TP),
            P(TP),
            P(TP),
            P(SP, TP),
            P(SP, TP),
        ),
        out_specs=P(SP, TP),
        check_vma=False,
    )
```

```python
from functools import partial

import jax
import jax.numpy as jnp
from jax import lax
from jax.experimental import pallas as pl
from jax.experimental.pallas import tpu as pltpu
from jax.sharding import Mesh
from jax.sharding import PartitionSpec as P

EPS = 1e-05
RES = 1.4142135623730951
SP = ("z", "y")
TP = ("x", "c")
ROWS = 768
HALF = 384
QUARTER = 192
TILE = 256
TILES = ROWS // TILE
HI = lax.Precision.HIGHEST
F32 = jnp.float32
BF = jnp.bfloat16


def vm():
    return pl.BlockSpec(memory_space=pltpu.VMEM)


def sm():
    return pl.BlockSpec(memory_space=pltpu.SMEM)


def near(a):
    return pltpu.with_memory_space_constraint(a, pltpu.VMEM)


def off(a):
    return pltpu.with_memory_space_constraint(a, pltpu.HBM)


def call(body, ins, outs, scratch=(), scalars=0, far=(), plain=()):
    run = pl.pallas_call(
        body,
        in_specs=[sm()] * scalars + [vm()] * (ins - scalars),
        out_specs=[vm()] * len(outs),
        out_shape=[(jax.ShapeDtypeStruct if k in plain else pltpu.VMEM)(*o) for k, o in enumerate(outs)],
        scratch_shapes=list(scratch),
        compiler_params=pltpu.CompilerParams(vmem_limit_bytes=24 * 2**20),
    )
    return lambda *a: run(*[off(b) if k in far else b if k < scalars else near(b) for k, b in enumerate(a)])


def iota(shape, dim):
    return lax.broadcasted_iota(jnp.int32, shape, dim)


def dot(a, b, ca, cb, precision=None):
    return lax.dot_general(
        a, b, (((ca,), (cb,)), ((), ())), precision=precision, preferred_element_type=F32
    )


def head_spread():
    return (iota((8, 512), 1) // 64 == iota((8, 512), 0)).astype(F32)


def conv_body(
    sp, rate, bias, v, e, r, lo, hi, tv, te, tr, step, sudden, doc,
    x_out, b_out, c_out, cum_out, dt_out, ct_out, dev_out, doc_out, si_out, pay_out, ext,
):
    base = sp[0] * 6
    rows = [doc[pl.ds(jnp.maximum(base - 1, 0), 1), :]]
    rows += [doc[pl.ds(base + k, 1), :] for k in range(6)]
    rows += [doc[pl.ds(jnp.minimum(base + 6, 191), 1), :]]
    lane = iota((1, 128), 1)
    first = jnp.where(sp[0] == 0, -1, rows[0])
    last = jnp.where(sp[0] == 31, -1, rows[7])
    window = jnp.concatenate([first] + rows[1:7] + [last], axis=1)
    own = window[:, 128:896]
    masks = []
    for d in range(-2, 3):
        moved = window if d == 0 else pltpu.roll(window, (-d) % 1024, 1)
        masks.append((moved[:, 128:896] == own).astype(F32))
    zero = jnp.zeros((1, ROWS), F32)
    mask_cols = jnp.transpose(jnp.concatenate(masks + [zero] * 3, axis=0))
    ext[8:776, 0:256] = v[...].astype(F32)
    ext[8:776, 256:384] = e[...].astype(F32)
    ext[8:776, 384:512] = r[...].astype(F32)
    ext[6:8, :] = lo[...].astype(F32)
    ext[776:778, :] = hi[...].astype(F32)
    taps = jnp.concatenate([tv[...], te[...], tr[...]], axis=1).astype(F32)
    acc = jnp.zeros((ROWS, 512), F32)
    for d in range(5):
        acc = acc + taps[d : d + 1, :] * (mask_cols[:, d : d + 1] * ext[6 + d : 6 + d + ROWS, :])
    act = acc * jax.nn.sigmoid(acc)
    x = act[:, 0:256]
    b = act[:, 256:384].astype(BF)
    x_out[...] = x.astype(BF)
    b_out[...] = b
    c_out[...] = act[:, 384:512].astype(BF)

    row = iota((8, 1), 0)
    fwd = row < 4
    rate_col = jnp.zeros((8, 1), F32)
    bias_col = jnp.zeros((8, 1), F32)
    for k in range(8):
        rate_col = jnp.where(row == k, rate[k // 4, k % 4], rate_col)
        bias_col = jnp.where(row == k, bias[k // 4, k % 4], bias_col)
    pick = (iota((8, 4), 0) % 4 == iota((8, 4), 1)).astype(F32)
    raw = dot(pick, step[...].astype(F32), 1, 1, HI) + bias_col
    dt = jnp.maximum(raw, 0.0) + jnp.log1p(jnp.exp(-jnp.abs(raw)))
    ld = -jnp.exp(rate_col) * dt + dot(pick, sudden[...], 1, 1, HI)
    dt_out[...] = dt
    dev = own.astype(F32)
    doc_out[...] = jnp.broadcast_to(dev, (8, ROWS))
    prev_id = window[:, 127:128].astype(F32)
    next_id = window[:, 896:897].astype(F32)
    upper = (iota((TILE, TILE), 0) <= iota((TILE, TILE), 1)).astype(F32)
    spread = head_spread()
    inc, exc, tot, dl, df = [], [], [], [], []
    for i in range(TILES):
        part = ld[:, i * TILE : (i + 1) * TILE]
        c = dot(part, upper, 1, 0, HI)
        inc.append(c)
        exc.append(c - part)
        tot.append(c[:, TILE - 1 : TILE])
        dl.append(dev[:, (i + 1) * TILE - 1 : (i + 1) * TILE])
        df.append(dev[:, i * TILE : i * TILE + 1])
    before = [prev_id, dl[0], dl[1]]
    after = [df[1], df[2], next_id]
    states, passing = [], []
    for i in range(TILES):
        ids = dev[:, i * TILE : (i + 1) * TILE]
        cols = slice(i * TILE, (i + 1) * TILE)
        cum_out[:, cols] = jnp.where(fwd, inc[i], exc[i])
        keep = ids == jnp.where(fwd, dl[i], df[i])
        weight = jnp.where(keep, dt[:, cols] * jnp.exp(jnp.where(fwd, tot[i] - inc[i], exc[i])), 0.0)
        wide = dot(weight, spread, 0, 0, HI)
        xi = x[i * TILE : (i + 1) * TILE, :]
        scaled = (jnp.concatenate([xi, xi], axis=1) * wide).astype(BF)
        states.append(dot(b[i * TILE : (i + 1) * TILE, :], scaled, 0, 0))
        reach = jnp.where(fwd, inc[i], tot[i] - exc[i])
        edge = jnp.where(fwd, before[i], after[i])
        ct_out[:, cols] = jnp.where(ids == edge, jnp.exp(reach), 0.0)
        far = jnp.where(fwd, sum(tot[:i], jnp.zeros((8, 1), F32)), sum(tot[i + 1 :], jnp.zeros((8, 1), F32)))
        dev_out[:, cols] = jnp.where(ids == jnp.where(fwd, prev_id, next_id), jnp.exp(reach + far), 0.0)
        through = jnp.where(jnp.where(fwd, dl[i], df[i]) == edge, jnp.exp(tot[i]), 0.0)
        passing.append(jnp.sum(through * spread, axis=0, keepdims=True))
    f = [s[:, 0:256] for s in states]
    g = [s[:, 256:512] for s in states]
    pf = [q[:, 0:256] for q in passing]
    pg = [q[:, 256:512] for q in passing]
    f2 = f[1] + pf[1] * f[0]
    g0 = g[1] + pg[1] * g[2]
    si_out[0] = f[0].astype(BF)
    si_out[1] = f2.astype(BF)
    si_out[2] = g0.astype(BF)
    si_out[3] = g[2].astype(BF)
    pay_out[0:128, 0:256] = (f[2] + pf[2] * f2).astype(BF)
    pay_out[0:128, 256:512] = (g[0] + pg[0] * g0).astype(BF)
    whole = passing[0] * passing[1] * passing[2]
    pay_out[128:144, :] = jnp.broadcast_to(whole, (16, 512)).astype(BF)


def local_body(x, b, c, cum, dt, ct, doc, si, y_out):
    spread = head_spread()
    lower = iota((TILE, TILE), 0) > iota((TILE, TILE), 1)
    upper = iota((TILE, TILE), 0) < iota((TILE, TILE), 1)
    side = iota((TILE, 128), 1) < 64
    for i in range(TILES):
        cols = slice(i * TILE, (i + 1) * TILE)
        cc = c[cols, :]
        score = dot(cc, b[cols, :], 1, 1)
        cum_row = cum[:, cols]
        cum_col = jnp.transpose(cum_row)
        ids = doc[:, cols]
        same = ids[0:1, :] == jnp.transpose(ids)[:, 0:1]
        score = jnp.where(same, score, 0.0)
        steps = dt[:, cols]
        carried = dot(ct[:, cols], spread, 0, 0, HI)
        for pair in range(2):
            xp = x[cols, pair * 128 : pair * 128 + 128]
            got = []
            for h in (2 * pair, 2 * pair + 1):
                spread_f = cum_col[:, h : h + 1] - cum_row[h : h + 1, :]
                spread_b = cum_row[h + 4 : h + 5, :] - cum_col[:, h + 4 : h + 5]
                reach = jnp.exp(jnp.where(upper, spread_b, spread_f))
                d0 = steps[h : h + 1, :]
                d1 = steps[h + 4 : h + 5, :]
                amount = jnp.where(lower, d0, jnp.where(upper, d1, d0 + d1))
                got.append(dot((score * (reach * amount)).astype(BF), xp, 1, 0))
            part = jnp.where(side, got[0], got[1])
            lanes = slice(pair * 128, pair * 128 + 128)
            wide = slice(256 + pair * 128, 384 + pair * 128)
            if i > 0:
                part = part + dot(cc, si[i - 1][:, lanes], 1, 0) * carried[:, lanes]
            if i < TILES - 1:
                part = part + dot(cc, si[i + 2][:, lanes], 1, 0) * carried[:, wide]
            y_out[cols, lanes] = part


def chain_body(where_y, pay, send_f, send_b, pre_out):
    y = where_y[0]
    for lanes, order, out in ((slice(0, 256), range(4), send_f), (slice(256, 512), range(3, -1, -1), send_b)):
        state = jnp.zeros((128, 256), F32)
        through = jnp.ones((1, 256), F32)
        pre, pre_through = state, through
        for k in order:
            pre = jnp.where(y == k, state, pre)
            pre_through = jnp.where(y == k, through, pre_through)
            hop = pay[k, 128:144, lanes].astype(F32)[0:1, :]
            state = state * hop + pay[k, 0:128, lanes].astype(F32)
            through = through * hop
        out[0:128, :] = state.astype(BF)
        out[128:144, :] = jnp.broadcast_to(through, (16, 256)).astype(BF)
        pre_out[0:128, lanes] = pre
        pre_out[128:136, lanes] = jnp.broadcast_to(pre_through, (8, 256))


def gate_body(core, yl, c, dev, pre, f1, f2, b1, b2, gate, gain, keep, send, normed):
    spread = head_spread()
    states = []
    for lanes, near, far in ((slice(0, 256), f1, f2), (slice(256, 512), b1, b2)):
        more = near[128:144, :].astype(F32)[0:1, :] * far[0:128, :].astype(F32)
        come = near[0:128, :].astype(F32) + more
        states.append((pre[0:128, lanes] + pre[128:129, lanes] * come).astype(BF))
    for i in range(TILES):
        cols = slice(i * TILE, (i + 1) * TILE)
        wide = dot(dev[:, cols], spread, 0, 0, HI)
        y = yl[cols, :]
        y = y + dot(c[cols, :], states[0], 1, 0) * wide[:, 0:256]
        y = y + dot(c[cols, :], states[1], 1, 0) * wide[:, 256:512]
        z = gate[cols, :].astype(F32)
        y = y * (z * jax.nn.sigmoid(z))
        y = y * lax.rsqrt(jnp.mean(y * y, axis=1, keepdims=True) + EPS)
        normed[cols, :] = (y * gain[...]).astype(BF)
    mine = pl.multiple_of(core[0] * HALF, HALF)
    other = pl.multiple_of(HALF - core[0] * HALF, HALF)
    keep[...] = normed[pl.ds(mine, HALF), :]
    send[...] = normed[pl.ds(other, HALF), :]


def mix_body(where_x, a, b, wa, wb, o0, o1, o2, o3):
    for k, out in ((2, o2), (1, o1), (3, o3), (0, o0)):
        block = pl.multiple_of(((where_x[0] + k) % 4) * 512, 512)
        got = dot(a[...], wa[:, pl.ds(block, 512)], 1, 0)
        got = got + dot(b[...], wb[:, pl.ds(block, 512)], 1, 0)
        out[...] = got.astype(BF)


def first_body(core, own, stream_a, stream_b, r1, r2, r3, gain_a, gain_b, out, total, gain):
    lane_a = pl.multiple_of(core[0] * 256, 256)
    lane_b = pl.multiple_of(256 - core[0] * 256, 256)
    total[:, pl.ds(lane_a, 256)] = stream_a[...].astype(F32)
    total[:, pl.ds(lane_b, 256)] = stream_b[...].astype(F32)
    gain[0:1, pl.ds(lane_a, 256)] = gain_a[0:1, :]
    gain[0:1, pl.ds(lane_b, 256)] = gain_b[0:1, :]
    mix = own[...].astype(F32) + r1[...].astype(F32) + r2[...].astype(F32) + r3[...].astype(F32)
    first = RES * total[...] + mix
    mean = jnp.mean(first, axis=1, keepdims=True).astype(BF).astype(F32)
    out[0:HALF, :] = (first - mean).astype(BF)
    means = jnp.transpose(jnp.broadcast_to(mean, (HALF, 128)))[0:1, :]
    means = jnp.concatenate([means, jnp.zeros((1, 128), F32)], axis=1)
    g = gain[0:1, :]
    g0 = g.astype(BF).astype(F32)
    g1 = (g - g0).astype(BF).astype(F32)
    g2 = g - g0 - g1
    row = iota((16, 512), 0)
    tail = jnp.where(row == 0, means, jnp.where(row == 1, g0, jnp.where(row == 2, g1, jnp.where(row == 3, g2, 0.0))))
    out[HALF : HALF + 16, :] = tail.astype(BF)


def up_body(where_x, p0, p1, p2, p3, w, hidden, resid, down, xn, up, sems):
    loads = []
    for core in range(2):
        for part in range(2):
            lanes = slice(part * 512, part * 512 + 512)
            loads.append((w.at[:, core, :, lanes], up.at[2 * core + part]))
    for block in range(4):
        rows = slice(block * 8, block * 8 + 8)
        loads.append((w.at[rows, :, :, 1024:2048], down.at[rows]))
    loads = [pltpu.make_async_copy(src, dst, sems.at[k]) for k, (src, dst) in enumerate(loads)]
    for load in loads:
        load.start()
    blocks = (p0, p1, p2, p3)
    tails = [p[HALF : HALF + 16, :].astype(F32) for p in blocks]
    means = jnp.concatenate([t[0:1, 0:HALF] for t in tails] + [jnp.zeros((4, HALF), F32)], axis=0)
    mean_cols = jnp.transpose(means)
    full = [p[0:HALF, :].astype(F32) + mean_cols[:, k : k + 1] for k, p in enumerate(blocks)]
    m = sum(jnp.sum(q, axis=1, keepdims=True) for q in full) / 2048.0
    full = [q - m for q in full]
    v = sum(jnp.sum(q * q, axis=1, keepdims=True) for q in full) / 2048.0
    scale = lax.rsqrt(v + EPS)
    for k, q in enumerate(full):
        gain = tails[k][1:2, :] + tails[k][2:3, :] + tails[k][3:4, :]
        done = (q * scale * gain).astype(BF)
        block = pl.multiple_of(((where_x[0] + (4 - k)) % 4) * 512, 512)
        xn[:, pl.ds(block, 512)] = done
        if k == 0:
            resid[...] = done
    for k in range(4):
        loads[k].wait()
        got = jnp.maximum(dot(xn[...], up[k].reshape(2048, 512), 1, 0), 0.0)
        hidden[:, k * 512 : k * 512 + 512] = (got * got).astype(BF)
    for k in range(4, 8):
        loads[k].wait()


def down_body(block, where_x, h, w, top, bottom):
    rows = pl.ds(((where_x[0] + block) % 4) * 8, 8)
    got = dot(h[:, 0:1024], w[rows, 0].reshape(512, 1024), 1, 1)
    got = (got + dot(h[:, 1024:2048], w[rows, 1].reshape(512, 1024), 1, 1)).astype(BF)
    top[...] = got[0:QUARTER]
    bottom[...] = got[QUARTER:]


def join_body(a, b, c, d, left, right):
    left[...] = (a[...].astype(F32) + b[...].astype(F32)).astype(BF)
    right[...] = (c[...].astype(F32) + d[...].astype(F32)).astype(BF)


def second_body(resid, own_top, own_bottom, top1, bottom1, top3, bottom3, second, stats):
    top = own_top[...].astype(F32) + top1[...].astype(F32) + top3[...].astype(F32)
    bottom = own_bottom[...].astype(F32) + bottom1[...].astype(F32) + bottom3[...].astype(F32)
    total = RES * resid[...].astype(F32) + jnp.concatenate([top, bottom], axis=0)
    second[...] = total
    s1 = jnp.transpose(jnp.broadcast_to(jnp.sum(total, axis=1, keepdims=True), (HALF, 128)))[0:8, :]
    s2 = jnp.transpose(jnp.broadcast_to(jnp.sum(total * total, axis=1, keepdims=True), (HALF, 128)))[0:8, :]
    stats[...] = jnp.where(iota((8, HALF), 0) == 0, s1, s2)


def last_body(core, second, s0, s1, s2, s3, gain_a, gain_b, full, send):
    stats = s0[...] + s1[...] + s2[...] + s3[...]
    cols = jnp.transpose(stats)
    m = cols[:, 0:1] / 2048.0
    v = cols[:, 1:2] / 2048.0 - m * m
    scale = lax.rsqrt(v + EPS)
    mine = pl.multiple_of(core[0] * 256, 256)
    other = pl.multiple_of(256 - core[0] * 256, 256)
    send[...] = ((second[:, pl.ds(other, 256)] - m) * scale * gain_b[1:2, :]).astype(BF)
    rows = pl.ds(pl.multiple_of(core[0] * HALF, HALF), HALF)
    full[rows, :] = ((second[:, pl.ds(mine, 256)] - m) * scale * gain_a[1:2, :]).astype(BF)


def layer(
    head_value_rows,
    entry_map_rows,
    readout_map_rows,
    output_gate_rows,
    step_before_softplus,
    sudden_log_decay,
    document_index,
    head_rate_logarithm,
    head_step_bias,
    value_conv_taps,
    entry_conv_taps,
    readout_conv_taps,
    group_norm_gain,
    mixer_output_weight,
    stream,
    mixer_norm_gain,
    channel_norm_gain,
    up_projection_weight,
    down_projection_weight,
):
    core = lax.axis_index("c")
    at_x = jnp.reshape(lax.axis_index("x"), (1,))
    at_c = jnp.reshape(core, (1,))
    at_y = jnp.reshape(lax.axis_index("y"), (1,))
    at_sp = jnp.reshape(lax.axis_index(SP), (1,))
    swap = [(0, 1), (1, 0)]

    def shift(a, axis, by, count):
        return lax.ppermute(a, axis, [(i, i + by) for i in range(count) if 0 <= i + by < count])

    def around(a, by):
        return lax.ppermute(a, "x", [(i, (i + by) % 4) for i in range(4)])

    tail = jnp.concatenate([a[ROWS - 2 :] for a in (head_value_rows, entry_map_rows, readout_map_rows)], axis=1)
    head = jnp.concatenate([a[:2] for a in (head_value_rows, entry_map_rows, readout_map_rows)], axis=1)
    low = shift(tail, SP, 1, 32)
    high = shift(head, SP, -1, 32)

    weights = jnp.concatenate([up_projection_weight, down_projection_weight], axis=1)
    weights = lax.all_gather(weights, ("z", "y", "c"), axis=0, tiled=True).reshape(32, 2, 64, 2048)

    weight_other = lax.ppermute(mixer_output_weight, "c", swap)
    stream_mine = lax.dynamic_slice_in_dim(stream, core * HALF, HALF)
    stream_other = lax.ppermute(lax.dynamic_slice_in_dim(stream, (1 - core) * HALF, HALF), "c", swap)
    gains = jnp.stack([mixer_norm_gain, channel_norm_gain])
    gains_other = lax.ppermute(gains, "c", swap)

    x, b, c, cum, dt, ct, dev, doc, si, pay = call(
        conv_body,
        14,
        [((ROWS, 256), BF), ((ROWS, 128), BF), ((ROWS, 128), BF)]
        + [((8, ROWS), F32)] * 5
        + [((4, 128, 256), BF), ((144, 512), BF)],
        scratch=[pltpu.VMEM((784, 512), F32)],
        scalars=3,
        far=(1, 2, 3, 4, 5, 8, 9, 10, 13),
    )(
        at_sp, head_rate_logarithm, head_step_bias, head_value_rows, entry_map_rows, readout_map_rows,
        low, high, value_conv_taps, entry_conv_taps, readout_conv_taps, step_before_softplus,
        sudden_log_decay, document_index.reshape(192, 128),
    )
    rows = lax.all_gather(pay, "y")
    send_f, send_b, pre = call(
        chain_body, 2, [((144, 256), BF), ((144, 256), BF), ((136, 512), F32)], scalars=1
    )(at_y, rows)
    f1, f2 = shift(send_f, "z", 1, 8), shift(send_f, "z", 2, 8)
    b1, b2 = shift(send_b, "z", -1, 8), shift(send_b, "z", -2, 8)
    yl = call(local_body, 8, [((ROWS, 256), F32)])(x, b, c, cum, dt, ct, doc, si)[0]
    keep, send = call(
        gate_body, 11, [((HALF, 256), BF)] * 2, scratch=[pltpu.VMEM((ROWS, 256), BF)], scalars=1, far=(9, 10)
    )(at_c, yl, c, dev, pre, f1, f2, b1, b2, output_gate_rows, group_norm_gain.reshape(1, 256))
    other = lax.ppermute(send, "c", swap)
    o0, o1, o2, o3 = call(mix_body, 5, [((HALF, 512), BF)] * 4, scalars=1, far=(3,))(
        at_x, keep, other, mixer_output_weight, weight_other
    )
    r2, r1, r3 = around(o2, 2), around(o1, 1), around(o3, 3)
    p0 = call(
        first_body,
        9,
        [((HALF + 16, 512), BF)],
        scratch=[pltpu.VMEM((HALF, 512), F32), pltpu.VMEM((8, 512), F32)],
        scalars=1,
    )(at_c, o0, stream_mine, stream_other, r1, r2, r3, gains, gains_other)[0]
    p2, p1, p3 = around(p0, 2), around(p0, 1), around(p0, 3)
    hidden, resid, down_weights = pl.pallas_call(
        up_body,
        in_specs=[sm()] + [vm()] * 4 + [pl.BlockSpec(memory_space=pltpu.HBM)],
        out_specs=[vm()] * 3,
        out_shape=[
            pltpu.VMEM((HALF, 2048), BF),
            pltpu.VMEM((HALF, 512), BF),
            pltpu.VMEM((32, 2, 64, 1024), BF),
        ],
        scratch_shapes=[
            pltpu.VMEM((HALF, 2048), BF),
            pltpu.VMEM((4, 32, 64, 512), BF),
            pltpu.SemaphoreType.DMA((8,)),
        ],
        compiler_params=pltpu.CompilerParams(vmem_limit_bytes=32 * 2**20),
        name="up",
    )(at_x, near(p0), near(p1), near(p2), near(p3), off(weights))

    def down(k):
        return call(partial(down_body, k), 3, [((QUARTER, 512), BF)] * 2, scalars=1)(at_x, hidden, down_weights)

    far_top, far_bottom = down(2)
    far_top, far_bottom = around(far_top, 1), around(far_bottom, 3)
    next_top, next_bottom = down(1)
    next_bottom = around(next_bottom, 1)
    back_top, back_bottom = down(3)
    back_top = around(back_top, 3)
    own_top, own_bottom = down(0)
    next_top, back_bottom = call(join_body, 4, [((QUARTER, 512), BF)] * 2)(next_top, far_top, back_bottom, far_bottom)
    next_top, back_bottom = around(next_top, 1), around(back_bottom, 3)
    second, stats = call(second_body, 7, [((HALF, 512), F32), ((8, HALF), F32)])(
        resid, own_top, own_bottom, next_top, next_bottom, back_top, back_bottom
    )
    s1, s2, s3 = around(stats, 1), around(stats, 2), around(stats, 3)
    full, send = call(last_body, 8, [((ROWS, 256), BF), ((HALF, 256), BF)], scalars=1, plain=(0,))(
        at_c, second, stats, s1, s2, s3, gains, gains_other
    )
    got = lax.ppermute(send, "c", swap)
    return lax.dynamic_update_slice_in_dim(full, got, (1 - core) * HALF, 0)


def solution(mesh):
    torus = Mesh(mesh.devices.reshape(8, 4, 4, 2), ("z", "y", "x", "c"))
    return jax.shard_map(
        layer,
        mesh=torus,
        in_specs=(
            P(SP, TP),
            P(SP, TP),
            P(SP, TP),
            P(SP, TP),
            P(SP, TP),
            P(SP, TP),
            P(),
            P(None, TP),
            P(None, TP),
            P(None, TP),
            P(None, TP),
            P(None, TP),
            P(TP),
            P(TP, None),
            P(SP, TP),
            P(TP),
            P(TP),
            P(SP, TP),
            P(SP, TP),
        ),
        out_specs=P(SP, TP),
        check_vma=False,
    )
```

```python
import jax
import jax.numpy as jnp
from jax import lax
from jax.experimental import pallas as pl
from jax.experimental.pallas import tpu as pltpu
from jax.sharding import Mesh
from jax.sharding import PartitionSpec as P

EPS = 1e-05
RES = 1.4142135623730951
SP = ("z", "y")
TP = ("x", "c")
ROWS = 768
HALF = 384
QUARTER = 192
TILE = 256
TILES = ROWS // TILE
HI = lax.Precision.HIGHEST
F32 = jnp.float32
BF = jnp.bfloat16


def vm():
    return pl.BlockSpec(memory_space=pltpu.VMEM)


def sm():
    return pl.BlockSpec(memory_space=pltpu.SMEM)


def near(a):
    return pltpu.with_memory_space_constraint(a, pltpu.VMEM)


def off(a):
    return pltpu.with_memory_space_constraint(a, pltpu.HBM)


def call(body, ins, outs, scratch=(), scalars=0, far=(), plain=()):
    run = pl.pallas_call(
        body,
        in_specs=[sm()] * scalars + [vm()] * (ins - scalars),
        out_specs=[vm()] * len(outs),
        out_shape=[(jax.ShapeDtypeStruct if k in plain else pltpu.VMEM)(*o) for k, o in enumerate(outs)],
        scratch_shapes=list(scratch),
        compiler_params=pltpu.CompilerParams(vmem_limit_bytes=24 * 2**20),
    )
    return lambda *a: run(*[off(b) if k in far else b if k < scalars else near(b) for k, b in enumerate(a)])


def iota(shape, dim):
    return lax.broadcasted_iota(jnp.int32, shape, dim)


def dot(a, b, ca, cb, precision=None):
    return lax.dot_general(
        a, b, (((ca,), (cb,)), ((), ())), precision=precision, preferred_element_type=F32
    )


def head_spread():
    return (iota((8, 512), 1) // 64 == iota((8, 512), 0)).astype(F32)


def conv_body(
    sp, rate, bias, v, e, r, lo, hi, tv, te, tr, step, sudden, doc,
    x_out, b_out, c_out, cum_out, dt_out, ct_out, dev_out, doc_out, si_out, pay_out, ext,
):
    base = sp[0] * 6
    rows = [doc[pl.ds(jnp.maximum(base - 1, 0), 1), :]]
    rows += [doc[pl.ds(base + k, 1), :] for k in range(6)]
    rows += [doc[pl.ds(jnp.minimum(base + 6, 191), 1), :]]
    lane = iota((1, 128), 1)
    first = jnp.where(sp[0] == 0, -1, rows[0])
    last = jnp.where(sp[0] == 31, -1, rows[7])
    window = jnp.concatenate([first] + rows[1:7] + [last], axis=1)
    own = window[:, 128:896]
    masks = []
    for d in range(-2, 3):
        moved = window if d == 0 else pltpu.roll(window, (-d) % 1024, 1)
        masks.append((moved[:, 128:896] == own).astype(F32))
    zero = jnp.zeros((1, ROWS), F32)
    mask_cols = jnp.transpose(jnp.concatenate(masks + [zero] * 3, axis=0))
    ext[8:776, 0:256] = v[...].astype(F32)
    ext[8:776, 256:384] = e[...].astype(F32)
    ext[8:776, 384:512] = r[...].astype(F32)
    ext[6:8, :] = lo[...].astype(F32)
    ext[776:778, :] = hi[...].astype(F32)
    taps = jnp.concatenate([tv[...], te[...], tr[...]], axis=1).astype(F32)
    acc = jnp.zeros((ROWS, 512), F32)
    for d in range(5):
        acc = acc + taps[d : d + 1, :] * (mask_cols[:, d : d + 1] * ext[6 + d : 6 + d + ROWS, :])
    act = acc * jax.nn.sigmoid(acc)
    x = act[:, 0:256]
    b = act[:, 256:384].astype(BF)
    x_out[...] = x.astype(BF)
    b_out[...] = b
    c_out[...] = act[:, 384:512].astype(BF)

    row = iota((8, 1), 0)
    fwd = row < 4
    rate_col = jnp.zeros((8, 1), F32)
    bias_col = jnp.zeros((8, 1), F32)
    for k in range(8):
        rate_col = jnp.where(row == k, rate[k // 4, k % 4], rate_col)
        bias_col = jnp.where(row == k, bias[k // 4, k % 4], bias_col)
    pick = (iota((8, 4), 0) % 4 == iota((8, 4), 1)).astype(F32)
    raw = dot(pick, step[...].astype(F32), 1, 1, HI) + bias_col
    dt = jnp.maximum(raw, 0.0) + jnp.log1p(jnp.exp(-jnp.abs(raw)))
    ld = -jnp.exp(rate_col) * dt + dot(pick, sudden[...], 1, 1, HI)
    dt_out[...] = dt
    dev = own.astype(F32)
    doc_out[...] = jnp.broadcast_to(dev, (8, ROWS))
    prev_id = window[:, 127:128].astype(F32)
    next_id = window[:, 896:897].astype(F32)
    upper = (iota((TILE, TILE), 0) <= iota((TILE, TILE), 1)).astype(F32)
    spread = head_spread()
    inc, exc, tot, dl, df = [], [], [], [], []
    for i in range(TILES):
        part = ld[:, i * TILE : (i + 1) * TILE]
        c = dot(part, upper, 1, 0, HI)
        inc.append(c)
        exc.append(c - part)
        tot.append(c[:, TILE - 1 : TILE])
        dl.append(dev[:, (i + 1) * TILE - 1 : (i + 1) * TILE])
        df.append(dev[:, i * TILE : i * TILE + 1])
    before = [prev_id, dl[0], dl[1]]
    after = [df[1], df[2], next_id]
    states, passing = [], []
    for i in range(TILES):
        ids = dev[:, i * TILE : (i + 1) * TILE]
        cols = slice(i * TILE, (i + 1) * TILE)
        cum_out[:, cols] = jnp.where(fwd, inc[i], exc[i])
        keep = ids == jnp.where(fwd, dl[i], df[i])
        weight = jnp.where(keep, dt[:, cols] * jnp.exp(jnp.where(fwd, tot[i] - inc[i], exc[i])), 0.0)
        wide = dot(weight, spread, 0, 0, HI)
        xi = x[i * TILE : (i + 1) * TILE, :]
        scaled = (jnp.concatenate([xi, xi], axis=1) * wide).astype(BF)
        states.append(dot(b[i * TILE : (i + 1) * TILE, :], scaled, 0, 0))
        reach = jnp.where(fwd, inc[i], tot[i] - exc[i])
        edge = jnp.where(fwd, before[i], after[i])
        ct_out[:, cols] = jnp.where(ids == edge, jnp.exp(reach), 0.0)
        far = jnp.where(fwd, sum(tot[:i], jnp.zeros((8, 1), F32)), sum(tot[i + 1 :], jnp.zeros((8, 1), F32)))
        dev_out[:, cols] = jnp.where(ids == jnp.where(fwd, prev_id, next_id), jnp.exp(reach + far), 0.0)
        through = jnp.where(jnp.where(fwd, dl[i], df[i]) == edge, jnp.exp(tot[i]), 0.0)
        passing.append(jnp.sum(through * spread, axis=0, keepdims=True))
    f = [s[:, 0:256] for s in states]
    g = [s[:, 256:512] for s in states]
    pf = [q[:, 0:256] for q in passing]
    pg = [q[:, 256:512] for q in passing]
    f2 = f[1] + pf[1] * f[0]
    g0 = g[1] + pg[1] * g[2]
    si_out[0] = jnp.zeros((128, 256), BF)
    si_out[1] = f[0].astype(BF)
    si_out[2] = f2.astype(BF)
    si_out[3] = g0.astype(BF)
    si_out[4] = g[2].astype(BF)
    si_out[5] = jnp.zeros((128, 256), BF)
    pay_out[0:128, 0:256] = (f[2] + pf[2] * f2).astype(BF)
    pay_out[0:128, 256:512] = (g[0] + pg[0] * g0).astype(BF)
    whole = passing[0] * passing[1] * passing[2]
    pay_out[128:144, :] = jnp.broadcast_to(whole, (16, 512)).astype(BF)


def local_body(x, b, c, cum, dt, ct, doc, si, y_out):
    spread = head_spread()
    lower = iota((TILE, TILE), 0) > iota((TILE, TILE), 1)
    upper = iota((TILE, TILE), 0) < iota((TILE, TILE), 1)
    side = iota((TILE, 128), 1) < 64

    @pl.loop(0, TILES)
    def _(i):
        cols = pl.ds(pl.multiple_of(i * TILE, TILE), TILE)
        cc = c[cols, :]
        score = dot(cc, b[cols, :], 1, 1)
        cum_row = cum[:, cols]
        cum_col = jnp.transpose(cum_row)
        ids = doc[:, cols]
        same = ids[0:1, :] == jnp.transpose(ids)[:, 0:1]
        score = jnp.where(same, score, 0.0)
        steps = dt[:, cols]
        carried = dot(ct[:, cols], spread, 0, 0, HI)
        for pair in range(2):
            xp = x[cols, pair * 128 : pair * 128 + 128]
            got = []
            for h in (2 * pair, 2 * pair + 1):
                spread_f = cum_col[:, h : h + 1] - cum_row[h : h + 1, :]
                spread_b = cum_row[h + 4 : h + 5, :] - cum_col[:, h + 4 : h + 5]
                reach = jnp.exp(jnp.where(upper, spread_b, spread_f))
                d0 = steps[h : h + 1, :]
                d1 = steps[h + 4 : h + 5, :]
                amount = jnp.where(lower, d0, jnp.where(upper, d1, d0 + d1))
                got.append(dot((score * (reach * amount)).astype(BF), xp, 1, 0))
            part = jnp.where(side, got[0], got[1])
            lanes = slice(pair * 128, pair * 128 + 128)
            wide = slice(256 + pair * 128, 384 + pair * 128)
            part = part + dot(cc, si[i, :, lanes], 1, 0) * carried[:, lanes]
            part = part + dot(cc, si[i + 3, :, lanes], 1, 0) * carried[:, wide]
            y_out[cols, lanes] = part


def chain_body(where_y, pay, send_f, send_b, pre_out):
    y = where_y[0]
    for lanes, order, out in ((slice(0, 256), range(4), send_f), (slice(256, 512), range(3, -1, -1), send_b)):
        state = jnp.zeros((128, 256), F32)
        through = jnp.ones((1, 256), F32)
        pre, pre_through = state, through
        for k in order:
            pre = jnp.where(y == k, state, pre)
            pre_through = jnp.where(y == k, through, pre_through)
            hop = pay[k, 128:144, lanes].astype(F32)[0:1, :]
            state = state * hop + pay[k, 0:128, lanes].astype(F32)
            through = through * hop
        out[0:128, :] = state.astype(BF)
        out[128:144, :] = jnp.broadcast_to(through, (16, 256)).astype(BF)
        pre_out[0:128, lanes] = pre
        pre_out[128:136, lanes] = jnp.broadcast_to(pre_through, (8, 256))


def gate_body(core, yl, c, dev, pre, f1, f2, b1, b2, gate, gain, keep, send, normed):
    spread = head_spread()
    states = []
    for lanes, near, far in ((slice(0, 256), f1, f2), (slice(256, 512), b1, b2)):
        more = near[128:144, :].astype(F32)[0:1, :] * far[0:128, :].astype(F32)
        come = near[0:128, :].astype(F32) + more
        states.append((pre[0:128, lanes] + pre[128:129, lanes] * come).astype(BF))

    @pl.loop(0, TILES)
    def _(i):
        cols = pl.ds(pl.multiple_of(i * TILE, TILE), TILE)
        wide = dot(dev[:, cols], spread, 0, 0, HI)
        y = yl[cols, :]
        y = y + dot(c[cols, :], states[0], 1, 0) * wide[:, 0:256]
        y = y + dot(c[cols, :], states[1], 1, 0) * wide[:, 256:512]
        z = gate[cols, :].astype(F32)
        y = y * (z * jax.nn.sigmoid(z))
        y = y * lax.rsqrt(jnp.mean(y * y, axis=1, keepdims=True) + EPS)
        normed[cols, :] = (y * gain[...]).astype(BF)

    mine = pl.multiple_of(core[0] * HALF, HALF)
    other = pl.multiple_of(HALF - core[0] * HALF, HALF)
    keep[...] = normed[pl.ds(mine, HALF), :]
    send[...] = normed[pl.ds(other, HALF), :]


def mix_body(where_x, a, b, wa, wb, o0, o1, o2, o3):
    for k, out in ((2, o2), (1, o1), (3, o3), (0, o0)):
        block = pl.multiple_of(((where_x[0] + k) % 4) * 512, 512)
        got = dot(a[...], wa[:, pl.ds(block, 512)], 1, 0)
        got = got + dot(b[...], wb[:, pl.ds(block, 512)], 1, 0)
        out[...] = got.astype(BF)


def first_body(core, own, stream_a, stream_b, r1, r2, r3, gain_a, gain_b, top, bottom, total, gain):
    lane_a = pl.multiple_of(core[0] * 256, 256)
    lane_b = pl.multiple_of(256 - core[0] * 256, 256)
    total[:, pl.ds(lane_a, 256)] = stream_a[...].astype(F32)
    total[:, pl.ds(lane_b, 256)] = stream_b[...].astype(F32)
    gain[0:1, pl.ds(lane_a, 256)] = gain_a[0:1, :]
    gain[0:1, pl.ds(lane_b, 256)] = gain_b[0:1, :]
    mix = own[...].astype(F32) + r1[...].astype(F32) + r2[...].astype(F32) + r3[...].astype(F32)
    first = RES * total[...] + mix
    mean = jnp.mean(first, axis=1, keepdims=True).astype(BF).astype(F32)
    centred = (first - mean).astype(BF)
    top[...] = centred[0:QUARTER]
    bottom[0:QUARTER, :] = centred[QUARTER:]
    means = jnp.transpose(jnp.broadcast_to(mean, (HALF, 128)))[0:1, :]
    means = jnp.concatenate([means, jnp.zeros((1, 128), F32)], axis=1)
    g = gain[0:1, :]
    g0 = g.astype(BF).astype(F32)
    g1 = (g - g0).astype(BF).astype(F32)
    g2 = g - g0 - g1
    row = iota((16, 512), 0)
    tail = jnp.where(row == 0, means, jnp.where(row == 1, g0, jnp.where(row == 2, g1, jnp.where(row == 3, g2, 0.0))))
    bottom[QUARTER : QUARTER + 16, :] = tail.astype(BF)


def rows_body(where_x, t0, b0, t1, b1, t2, b2, t3, b3, xn, resid):
    blocks = ((t0, b0), (t1, b1), (t2, b2), (t3, b3))
    tails = [b[QUARTER : QUARTER + 16, :].astype(F32) for _, b in blocks]
    means = jnp.concatenate([t[0:1, 0:HALF] for t in tails] + [jnp.zeros((4, HALF), F32)], axis=0)
    mean_cols = jnp.transpose(means)
    full = [
        jnp.concatenate([t[...], b[0:QUARTER, :]], axis=0).astype(F32) + mean_cols[:, k : k + 1]
        for k, (t, b) in enumerate(blocks)
    ]
    m = sum(jnp.sum(q, axis=1, keepdims=True) for q in full) / 2048.0
    full = [q - m for q in full]
    v = sum(jnp.sum(q * q, axis=1, keepdims=True) for q in full) / 2048.0
    scale = lax.rsqrt(v + EPS)
    for k, q in enumerate(full):
        gain = tails[k][1:2, :] + tails[k][2:3, :] + tails[k][3:4, :]
        done = (q * scale * gain).astype(BF)
        block = pl.multiple_of(((where_x[0] + (4 - k)) % 4) * 512, 512)
        xn[:, pl.ds(block, 512)] = done
        if k == 0:
            resid[...] = done


CHUNKS = 4


def rows_of(w, where_x, block, to, sems):
    loads = []
    for k in range(2):
        rows = pl.ds(((where_x[0] + block) % 4) * 8 + 4 * k, 4)
        loads.append(pltpu.make_async_copy(w.at[rows, :, :, pl.ds(1024, 1024)], to.at[pl.ds(4 * k, 4)], sems[k]))
    return loads


def up_body(where_x, xn, w, hidden, far, after, back, up, sems):
    loads = []
    for k in range(CHUNKS):
        src = w.at[:, k // 2, :, pl.ds((k % 2) * 512, 512)]
        loads.append(pltpu.make_async_copy(src, up.at[k], sems.at[k]))
    for j, (block, to) in enumerate(((2, far), (1, after), (3, back))):
        loads += rows_of(w, where_x, block, to, [sems.at[CHUNKS + 2 * j], sems.at[CHUNKS + 2 * j + 1]])
    for load in loads:
        load.start()

    @pl.loop(0, CHUNKS)
    def _(k):
        pltpu.make_async_copy(up.at[k], up.at[k], sems.at[k]).wait()
        got = jnp.maximum(dot(xn[...], up[k].reshape(2048, 512), 1, 0), 0.0)
        hidden[:, pl.ds(pl.multiple_of(k * 512, 512), 512)] = (got * got).astype(BF)

    for load in loads[CHUNKS:]:
        load.wait()


def own_body(where_x, h, source, top, bottom, w, sems):
    loads = rows_of(source, where_x, 0, w, [sems.at[0], sems.at[1]])
    for load in loads:
        load.start()
    for load in loads:
        load.wait()
    down_body(h, w, top, bottom)


def down_body(h, w, top, bottom):
    got = dot(h[:, 0:1024], w[:, 0].reshape(512, 1024), 1, 1)
    got = (got + dot(h[:, 1024:2048], w[:, 1].reshape(512, 1024), 1, 1)).astype(BF)
    top[...] = got[0:QUARTER]
    bottom[...] = got[QUARTER:]


def join_body(a, b, c, d, left, right):
    left[...] = (a[...].astype(F32) + b[...].astype(F32)).astype(BF)
    right[...] = (c[...].astype(F32) + d[...].astype(F32)).astype(BF)


def second_body(resid, own_top, own_bottom, top1, bottom1, top3, bottom3, second, stats):
    top = own_top[...].astype(F32) + top1[...].astype(F32) + top3[...].astype(F32)
    bottom = own_bottom[...].astype(F32) + bottom1[...].astype(F32) + bottom3[...].astype(F32)
    total = RES * resid[...].astype(F32) + jnp.concatenate([top, bottom], axis=0)
    second[...] = total
    s1 = jnp.transpose(jnp.broadcast_to(jnp.sum(total, axis=1, keepdims=True), (HALF, 128)))[0:8, :]
    s2 = jnp.transpose(jnp.broadcast_to(jnp.sum(total * total, axis=1, keepdims=True), (HALF, 128)))[0:8, :]
    stats[...] = jnp.where(iota((8, HALF), 0) == 0, s1, s2)


def last_body(core, second, s0, s1, s2, s3, gain_a, gain_b, full, send):
    stats = s0[...] + s1[...] + s2[...] + s3[...]
    cols = jnp.transpose(stats)
    m = cols[:, 0:1] / 2048.0
    v = cols[:, 1:2] / 2048.0 - m * m
    scale = lax.rsqrt(v + EPS)
    mine = pl.multiple_of(core[0] * 256, 256)
    other = pl.multiple_of(256 - core[0] * 256, 256)
    send[...] = ((second[:, pl.ds(other, 256)] - m) * scale * gain_b[1:2, :]).astype(BF)
    rows = pl.ds(pl.multiple_of(core[0] * HALF, HALF), HALF)
    full[rows, :] = ((second[:, pl.ds(mine, 256)] - m) * scale * gain_a[1:2, :]).astype(BF)


def layer(
    head_value_rows,
    entry_map_rows,
    readout_map_rows,
    output_gate_rows,
    step_before_softplus,
    sudden_log_decay,
    document_index,
    head_rate_logarithm,
    head_step_bias,
    value_conv_taps,
    entry_conv_taps,
    readout_conv_taps,
    group_norm_gain,
    mixer_output_weight,
    stream,
    mixer_norm_gain,
    channel_norm_gain,
    up_projection_weight,
    down_projection_weight,
):
    core = lax.axis_index("c")
    at_x = jnp.reshape(lax.axis_index("x"), (1,))
    at_c = jnp.reshape(core, (1,))
    at_y = jnp.reshape(lax.axis_index("y"), (1,))
    at_sp = jnp.reshape(lax.axis_index(SP), (1,))
    swap = [(0, 1), (1, 0)]

    def shift(a, axis, by, count):
        return lax.ppermute(a, axis, [(i, i + by) for i in range(count) if 0 <= i + by < count])

    def around(a, by):
        return lax.ppermute(a, "x", [(i, (i + by) % 4) for i in range(4)])

    tail = jnp.concatenate([a[ROWS - 2 :] for a in (head_value_rows, entry_map_rows, readout_map_rows)], axis=1)
    head = jnp.concatenate([a[:2] for a in (head_value_rows, entry_map_rows, readout_map_rows)], axis=1)
    low = shift(tail, SP, 1, 32)
    high = shift(head, SP, -1, 32)

    weights = jnp.concatenate([up_projection_weight, down_projection_weight], axis=1)
    weights = lax.all_gather(weights, ("z", "y", "c"), axis=0, tiled=True).reshape(32, 2, 64, 2048)

    weight_other = lax.ppermute(mixer_output_weight, "c", swap)
    stream_mine = lax.dynamic_slice_in_dim(stream, core * HALF, HALF)
    stream_other = lax.ppermute(lax.dynamic_slice_in_dim(stream, (1 - core) * HALF, HALF), "c", swap)
    gains = jnp.stack([mixer_norm_gain, channel_norm_gain])
    gains_other = lax.ppermute(gains, "c", swap)

    x, b, c, cum, dt, ct, dev, doc, si, pay = call(
        conv_body,
        14,
        [((ROWS, 256), BF), ((ROWS, 128), BF), ((ROWS, 128), BF)]
        + [((8, ROWS), F32)] * 5
        + [((6, 128, 256), BF), ((144, 512), BF)],
        scratch=[pltpu.VMEM((784, 512), F32)],
        scalars=3,
        far=(1, 2, 3, 4, 5, 8, 9, 10, 13),
    )(
        at_sp, head_rate_logarithm, head_step_bias, head_value_rows, entry_map_rows, readout_map_rows,
        low, high, value_conv_taps, entry_conv_taps, readout_conv_taps, step_before_softplus,
        sudden_log_decay, document_index.reshape(192, 128),
    )
    rows = lax.all_gather(pay, "y")
    send_f, send_b, pre = call(
        chain_body, 2, [((144, 256), BF), ((144, 256), BF), ((136, 512), F32)], scalars=1
    )(at_y, rows)
    f1, f2 = shift(send_f, "z", 1, 8), shift(send_f, "z", 2, 8)
    b1, b2 = shift(send_b, "z", -1, 8), shift(send_b, "z", -2, 8)
    yl = call(local_body, 8, [((ROWS, 256), F32)])(x, b, c, cum, dt, ct, doc, si)[0]
    keep, send = call(
        gate_body, 11, [((HALF, 256), BF)] * 2, scratch=[pltpu.VMEM((ROWS, 256), BF)], scalars=1, far=(9, 10)
    )(at_c, yl, c, dev, pre, f1, f2, b1, b2, output_gate_rows, group_norm_gain.reshape(1, 256))
    other = lax.ppermute(send, "c", swap)
    o0, o1, o2, o3 = call(mix_body, 5, [((HALF, 512), BF)] * 4, scalars=1, far=(3,))(
        at_x, keep, other, mixer_output_weight, weight_other
    )
    r2, r1, r3 = around(o2, 2), around(o1, 1), around(o3, 3)
    top, bottom = call(
        first_body,
        9,
        [((QUARTER, 512), BF), ((QUARTER + 16, 512), BF)],
        scratch=[pltpu.VMEM((HALF, 512), F32), pltpu.VMEM((8, 512), F32)],
        scalars=1,
    )(at_c, o0, stream_mine, stream_other, r1, r2, r3, gains, gains_other)
    top1, bottom3 = around(top, 1), around(bottom, 3)
    top3, bottom1 = around(top, 3), around(bottom, 1)
    top2, bottom2 = around(top1, 1), around(bottom3, 3)
    rows, resid = call(rows_body, 9, [((HALF, 2048), BF), ((HALF, 512), BF)], scalars=1)(
        at_x, top, bottom, top1, bottom1, top2, bottom2, top3, bottom3
    )
    hidden, part2, part1, part3 = pl.pallas_call(
        up_body,
        in_specs=[sm(), vm(), pl.BlockSpec(memory_space=pltpu.HBM)],
        out_specs=[vm()] * 4,
        out_shape=[pltpu.VMEM((HALF, 2048), BF)] + [pltpu.VMEM((8, 2, 64, 1024), BF)] * 3,
        scratch_shapes=[
            pltpu.VMEM((CHUNKS, 32, 64, 2048 // CHUNKS), BF),
            pltpu.SemaphoreType.DMA((CHUNKS + 6,)),
        ],
        compiler_params=pltpu.CompilerParams(vmem_limit_bytes=32 * 2**20),
        name="up",
    )(at_x, near(rows), off(weights))

    def down(part):
        return call(down_body, 2, [((QUARTER, 512), BF)] * 2)(hidden, part)

    far_top, far_bottom = down(part2)
    far_top, far_bottom = around(far_top, 1), around(far_bottom, 3)
    next_top, next_bottom = down(part1)
    next_bottom = around(next_bottom, 1)
    back_top, back_bottom = down(part3)
    back_top = around(back_top, 3)
    own_top, own_bottom = pl.pallas_call(
        own_body,
        in_specs=[sm(), vm(), pl.BlockSpec(memory_space=pltpu.HBM)],
        out_specs=[vm()] * 2,
        out_shape=[pltpu.VMEM((QUARTER, 512), BF)] * 2,
        scratch_shapes=[pltpu.VMEM((8, 2, 64, 1024), BF), pltpu.SemaphoreType.DMA((2,))],
        compiler_params=pltpu.CompilerParams(vmem_limit_bytes=24 * 2**20),
        name="down0",
    )(at_x, near(hidden), off(weights))
    next_top, back_bottom = call(join_body, 4, [((QUARTER, 512), BF)] * 2)(next_top, far_top, back_bottom, far_bottom)
    next_top, back_bottom = around(next_top, 1), around(back_bottom, 3)
    second, stats = call(second_body, 7, [((HALF, 512), F32), ((8, HALF), F32)])(
        resid, own_top, own_bottom, next_top, next_bottom, back_top, back_bottom
    )
    s1, s2, s3 = around(stats, 1), around(stats, 2), around(stats, 3)
    full, send = call(last_body, 8, [((ROWS, 256), BF), ((HALF, 256), BF)], scalars=1, plain=(0,))(
        at_c, second, stats, s1, s2, s3, gains, gains_other
    )
    got = lax.ppermute(send, "c", swap)
    return lax.dynamic_update_slice_in_dim(full, got, (1 - core) * HALF, 0)


def solution(mesh):
    torus = Mesh(mesh.devices.reshape(8, 4, 4, 2), ("z", "y", "x", "c"))
    return jax.shard_map(
        layer,
        mesh=torus,
        in_specs=(
            P(SP, TP),
            P(SP, TP),
            P(SP, TP),
            P(SP, TP),
            P(SP, TP),
            P(SP, TP),
            P(),
            P(None, TP),
            P(None, TP),
            P(None, TP),
            P(None, TP),
            P(None, TP),
            P(TP),
            P(TP, None),
            P(SP, TP),
            P(TP),
            P(TP),
            P(SP, TP),
            P(SP, TP),
        ),
        out_specs=P(SP, TP),
        check_vma=False,
    )
```

```python
import jax
import jax.numpy as jnp
from jax import lax
from jax.experimental import pallas as pl
from jax.experimental.pallas import tpu as pltpu
from jax.sharding import Mesh
from jax.sharding import PartitionSpec as P

EPS = 1e-05
RES = 1.4142135623730951
SP = ("z", "y")
TP = ("x", "c")
ROWS = 768
HALF = 384
QUARTER = 192
TILE = 256
TILES = ROWS // TILE
HI = lax.Precision.HIGHEST
F32 = jnp.float32
BF = jnp.bfloat16


def vm():
    return pl.BlockSpec(memory_space=pltpu.VMEM)


def sm():
    return pl.BlockSpec(memory_space=pltpu.SMEM)


def near(a):
    return pltpu.with_memory_space_constraint(a, pltpu.VMEM)


def off(a):
    return pltpu.with_memory_space_constraint(a, pltpu.HBM)


def call(body, ins, outs, scratch=(), scalars=0, far=(), plain=()):
    run = pl.pallas_call(
        body,
        in_specs=[sm()] * scalars + [vm()] * (ins - scalars),
        out_specs=[vm()] * len(outs),
        out_shape=[(jax.ShapeDtypeStruct if k in plain else pltpu.VMEM)(*o) for k, o in enumerate(outs)],
        scratch_shapes=list(scratch),
        compiler_params=pltpu.CompilerParams(vmem_limit_bytes=24 * 2**20),
    )
    return lambda *a: run(*[off(b) if k in far else b if k < scalars else near(b) for k, b in enumerate(a)])


def iota(shape, dim):
    return lax.broadcasted_iota(jnp.int32, shape, dim)


def dot(a, b, ca, cb, precision=None):
    return lax.dot_general(
        a, b, (((ca,), (cb,)), ((), ())), precision=precision, preferred_element_type=F32
    )


def head_spread():
    return (iota((8, 512), 1) // 64 == iota((8, 512), 0)).astype(F32)


def conv_body(
    sp, rate, bias, v, e, r, lo, hi, tv, te, tr, step, sudden, doc,
    x_out, b_out, c_out, cum_out, dt_out, ct_out, dev_out, doc_out, si_out, pay_out, ext,
):
    base = sp[0] * 6
    rows = [doc[pl.ds(jnp.maximum(base - 1, 0), 1), :]]
    rows += [doc[pl.ds(base + k, 1), :] for k in range(6)]
    rows += [doc[pl.ds(jnp.minimum(base + 6, 191), 1), :]]
    lane = iota((1, 128), 1)
    first = jnp.where(sp[0] == 0, -1, rows[0])
    last = jnp.where(sp[0] == 31, -1, rows[7])
    window = jnp.concatenate([first] + rows[1:7] + [last], axis=1)
    own = window[:, 128:896]
    masks = []
    for d in range(-2, 3):
        moved = window if d == 0 else pltpu.roll(window, (-d) % 1024, 1)
        masks.append((moved[:, 128:896] == own).astype(F32))
    zero = jnp.zeros((1, ROWS), F32)
    mask_cols = jnp.transpose(jnp.concatenate(masks + [zero] * 3, axis=0))
    ext[8:776, 0:256] = v[...].astype(F32)
    ext[8:776, 256:384] = e[...].astype(F32)
    ext[8:776, 384:512] = r[...].astype(F32)
    ext[6:8, :] = lo[...].astype(F32)
    ext[776:778, :] = hi[...].astype(F32)
    taps = jnp.concatenate([tv[...], te[...], tr[...]], axis=1).astype(F32)
    acc = jnp.zeros((ROWS, 512), F32)
    for d in range(5):
        acc = acc + taps[d : d + 1, :] * (mask_cols[:, d : d + 1] * ext[6 + d : 6 + d + ROWS, :])
    act = acc * jax.nn.sigmoid(acc)
    x = act[:, 0:256]
    b = act[:, 256:384].astype(BF)
    x_out[...] = x.astype(BF)
    b_out[...] = b
    c_out[...] = act[:, 384:512].astype(BF)

    row = iota((8, 1), 0)
    fwd = row < 4
    rate_col = jnp.zeros((8, 1), F32)
    bias_col = jnp.zeros((8, 1), F32)
    for k in range(8):
        rate_col = jnp.where(row == k, rate[k // 4, k % 4], rate_col)
        bias_col = jnp.where(row == k, bias[k // 4, k % 4], bias_col)
    pick = (iota((8, 4), 0) % 4 == iota((8, 4), 1)).astype(F32)
    raw = dot(pick, step[...].astype(F32), 1, 1, HI) + bias_col
    dt = jnp.maximum(raw, 0.0) + jnp.log1p(jnp.exp(-jnp.abs(raw)))
    ld = -jnp.exp(rate_col) * dt + dot(pick, sudden[...], 1, 1, HI)
    dt_out[...] = dt
    dev = own.astype(F32)
    doc_out[...] = jnp.broadcast_to(dev, (8, ROWS))
    prev_id = window[:, 127:128].astype(F32)
    next_id = window[:, 896:897].astype(F32)
    upper = (iota((TILE, TILE), 0) <= iota((TILE, TILE), 1)).astype(F32)
    spread = head_spread()
    inc, exc, tot, dl, df = [], [], [], [], []
    for i in range(TILES):
        part = ld[:, i * TILE : (i + 1) * TILE]
        c = dot(part, upper, 1, 0, HI)
        inc.append(c)
        exc.append(c - part)
        tot.append(c[:, TILE - 1 : TILE])
        dl.append(dev[:, (i + 1) * TILE - 1 : (i + 1) * TILE])
        df.append(dev[:, i * TILE : i * TILE + 1])
    before = [prev_id, dl[0], dl[1]]
    after = [df[1], df[2], next_id]
    states, passing = [], []
    for i in range(TILES):
        ids = dev[:, i * TILE : (i + 1) * TILE]
        cols = slice(i * TILE, (i + 1) * TILE)
        cum_out[:, cols] = jnp.where(fwd, inc[i], exc[i])
        keep = ids == jnp.where(fwd, dl[i], df[i])
        weight = jnp.where(keep, dt[:, cols] * jnp.exp(jnp.where(fwd, tot[i] - inc[i], exc[i])), 0.0)
        wide = dot(weight, spread, 0, 0, HI)
        xi = x[i * TILE : (i + 1) * TILE, :]
        scaled = (jnp.concatenate([xi, xi], axis=1) * wide).astype(BF)
        states.append(dot(b[i * TILE : (i + 1) * TILE, :], scaled, 0, 0))
        reach = jnp.where(fwd, inc[i], tot[i] - exc[i])
        edge = jnp.where(fwd, before[i], after[i])
        ct_out[:, cols] = jnp.where(ids == edge, jnp.exp(reach), 0.0)
        far = jnp.where(fwd, sum(tot[:i], jnp.zeros((8, 1), F32)), sum(tot[i + 1 :], jnp.zeros((8, 1), F32)))
        dev_out[:, cols] = jnp.where(ids == jnp.where(fwd, prev_id, next_id), jnp.exp(reach + far), 0.0)
        through = jnp.where(jnp.where(fwd, dl[i], df[i]) == edge, jnp.exp(tot[i]), 0.0)
        passing.append(jnp.sum(through * spread, axis=0, keepdims=True))
    f = [s[:, 0:256] for s in states]
    g = [s[:, 256:512] for s in states]
    pf = [q[:, 0:256] for q in passing]
    pg = [q[:, 256:512] for q in passing]
    f2 = f[1] + pf[1] * f[0]
    g0 = g[1] + pg[1] * g[2]
    si_out[0] = jnp.zeros((128, 256), BF)
    si_out[1] = f[0].astype(BF)
    si_out[2] = f2.astype(BF)
    si_out[3] = g0.astype(BF)
    si_out[4] = g[2].astype(BF)
    si_out[5] = jnp.zeros((128, 256), BF)
    pay_out[0:128, 0:256] = (f[2] + pf[2] * f2).astype(BF)
    pay_out[0:128, 256:512] = (g[0] + pg[0] * g0).astype(BF)
    whole = passing[0] * passing[1] * passing[2]
    pay_out[128:144, :] = jnp.broadcast_to(whole, (16, 512)).astype(BF)


def local_body(x, b, c, cum, dt, ct, doc, si, y_out):
    spread = head_spread()
    lower = iota((TILE, TILE), 0) > iota((TILE, TILE), 1)
    upper = iota((TILE, TILE), 0) < iota((TILE, TILE), 1)
    side = iota((TILE, 128), 1) < 64

    @pl.loop(0, TILES)
    def _(i):
        cols = pl.ds(pl.multiple_of(i * TILE, TILE), TILE)
        cc = c[cols, :]
        score = dot(cc, b[cols, :], 1, 1)
        cum_row = cum[:, cols]
        cum_col = jnp.transpose(cum_row)
        ids = doc[:, cols]
        same = ids[0:1, :] == jnp.transpose(ids)[:, 0:1]
        score = jnp.where(same, score, 0.0)
        steps = dt[:, cols]
        carried = dot(ct[:, cols], spread, 0, 0, HI)
        for pair in range(2):
            xp = x[cols, pair * 128 : pair * 128 + 128]
            got = []
            for h in (2 * pair, 2 * pair + 1):
                spread_f = cum_col[:, h : h + 1] - cum_row[h : h + 1, :]
                spread_b = cum_row[h + 4 : h + 5, :] - cum_col[:, h + 4 : h + 5]
                reach = jnp.exp(jnp.where(upper, spread_b, spread_f))
                d0 = steps[h : h + 1, :]
                d1 = steps[h + 4 : h + 5, :]
                amount = jnp.where(lower, d0, jnp.where(upper, d1, d0 + d1))
                got.append(dot((score * (reach * amount)).astype(BF), xp, 1, 0))
            part = jnp.where(side, got[0], got[1])
            lanes = slice(pair * 128, pair * 128 + 128)
            wide = slice(256 + pair * 128, 384 + pair * 128)
            part = part + dot(cc, si[i, :, lanes], 1, 0) * carried[:, lanes]
            part = part + dot(cc, si[i + 3, :, lanes], 1, 0) * carried[:, wide]
            y_out[cols, lanes] = part


def chain_body(where_y, pay, send_f, send_b, pre_out):
    y = where_y[0]
    for lanes, order, out in ((slice(0, 256), range(4), send_f), (slice(256, 512), range(3, -1, -1), send_b)):
        state = jnp.zeros((128, 256), F32)
        through = jnp.ones((1, 256), F32)
        pre, pre_through = state, through
        for k in order:
            pre = jnp.where(y == k, state, pre)
            pre_through = jnp.where(y == k, through, pre_through)
            hop = pay[k, 128:144, lanes].astype(F32)[0:1, :]
            state = state * hop + pay[k, 0:128, lanes].astype(F32)
            through = through * hop
        out[0:128, :] = state.astype(BF)
        out[128:144, :] = jnp.broadcast_to(through, (16, 256)).astype(BF)
        pre_out[0:128, lanes] = pre
        pre_out[128:136, lanes] = jnp.broadcast_to(pre_through, (8, 256))


def gate_body(core, yl, c, dev, pre, f1, f2, b1, b2, gate, gain, keep, send, normed):
    spread = head_spread()
    states = []
    for lanes, near, far in ((slice(0, 256), f1, f2), (slice(256, 512), b1, b2)):
        more = near[128:144, :].astype(F32)[0:1, :] * far[0:128, :].astype(F32)
        come = near[0:128, :].astype(F32) + more
        states.append((pre[0:128, lanes] + pre[128:129, lanes] * come).astype(BF))

    @pl.loop(0, TILES)
    def _(i):
        cols = pl.ds(pl.multiple_of(i * TILE, TILE), TILE)
        wide = dot(dev[:, cols], spread, 0, 0, HI)
        y = yl[cols, :]
        y = y + dot(c[cols, :], states[0], 1, 0) * wide[:, 0:256]
        y = y + dot(c[cols, :], states[1], 1, 0) * wide[:, 256:512]
        z = gate[cols, :].astype(F32)
        y = y * (z * jax.nn.sigmoid(z))
        y = y * lax.rsqrt(jnp.mean(y * y, axis=1, keepdims=True) + EPS)
        normed[cols, :] = (y * gain[...]).astype(BF)

    mine = pl.multiple_of(core[0] * HALF, HALF)
    other = pl.multiple_of(HALF - core[0] * HALF, HALF)
    keep[...] = normed[pl.ds(mine, HALF), :]
    send[...] = normed[pl.ds(other, HALF), :]


def mix_body(where_x, a, b, wa, wb, o0, o1, o2, o3):
    for k, out in ((2, o2), (1, o1), (3, o3), (0, o0)):
        block = pl.multiple_of(((where_x[0] + k) % 4) * 512, 512)
        got = dot(a[...], wa[:, pl.ds(block, 512)], 1, 0)
        got = got + dot(b[...], wb[:, pl.ds(block, 512)], 1, 0)
        out[...] = got.astype(BF)


def first_body(core, own, stream_a, stream_b, r1, r2, r3, gain_a, gain_b, top, bottom, total, gain):
    lane_a = pl.multiple_of(core[0] * 256, 256)
    lane_b = pl.multiple_of(256 - core[0] * 256, 256)
    total[:, pl.ds(lane_a, 256)] = stream_a[...].astype(F32)
    total[:, pl.ds(lane_b, 256)] = stream_b[...].astype(F32)
    gain[0:1, pl.ds(lane_a, 256)] = gain_a[0:1, :]
    gain[0:1, pl.ds(lane_b, 256)] = gain_b[0:1, :]
    mix = own[...].astype(F32) + r1[...].astype(F32) + r2[...].astype(F32) + r3[...].astype(F32)
    first = RES * total[...] + mix
    mean = jnp.mean(first, axis=1, keepdims=True).astype(BF).astype(F32)
    centred = (first - mean).astype(BF)
    top[...] = centred[0:QUARTER]
    bottom[0:QUARTER, :] = centred[QUARTER:]
    means = jnp.transpose(jnp.broadcast_to(mean, (HALF, 128)))[0:1, :]
    means = jnp.concatenate([means, jnp.zeros((1, 128), F32)], axis=1)
    g = gain[0:1, :]
    g0 = g.astype(BF).astype(F32)
    g1 = (g - g0).astype(BF).astype(F32)
    g2 = g - g0 - g1
    row = iota((16, 512), 0)
    tail = jnp.where(row == 0, means, jnp.where(row == 1, g0, jnp.where(row == 2, g1, jnp.where(row == 3, g2, 0.0))))
    bottom[QUARTER : QUARTER + 16, :] = tail.astype(BF)


def rows_body(where_x, t0, b0, t1, b1, t2, b2, t3, b3, xn, resid):
    blocks = ((t0, b0), (t1, b1), (t2, b2), (t3, b3))
    tails = [b[QUARTER : QUARTER + 16, :].astype(F32) for _, b in blocks]
    means = jnp.concatenate([t[0:1, 0:HALF] for t in tails] + [jnp.zeros((4, HALF), F32)], axis=0)
    mean_cols = jnp.transpose(means)
    full = [
        jnp.concatenate([t[...], b[0:QUARTER, :]], axis=0).astype(F32) + mean_cols[:, k : k + 1]
        for k, (t, b) in enumerate(blocks)
    ]
    m = sum(jnp.sum(q, axis=1, keepdims=True) for q in full) / 2048.0
    full = [q - m for q in full]
    v = sum(jnp.sum(q * q, axis=1, keepdims=True) for q in full) / 2048.0
    scale = lax.rsqrt(v + EPS)
    for k, q in enumerate(full):
        gain = tails[k][1:2, :] + tails[k][2:3, :] + tails[k][3:4, :]
        done = (q * scale * gain).astype(BF)
        block = pl.multiple_of(((where_x[0] + (4 - k)) % 4) * 512, 512)
        xn[:, pl.ds(block, 512)] = done
        if k == 0:
            resid[...] = done


CHUNKS = 4


def rows_of(w, where_x, block, to, sems):
    loads = []
    for k in range(2):
        rows = pl.ds(((where_x[0] + block) % 4) * 8 + 4 * k, 4)
        loads.append(pltpu.make_async_copy(w.at[rows, :, :, pl.ds(1024, 1024)], to.at[pl.ds(4 * k, 4)], sems[k]))
    return loads


def up_body(where_x, xn, w, hidden, after, back, top, bottom, far, up, sems):
    loads = []
    for k in range(CHUNKS):
        src = w.at[:, k // 2, :, pl.ds((k % 2) * 512, 512)]
        loads.append(pltpu.make_async_copy(src, up.at[k], sems.at[k]))
    for j, (block, to) in enumerate(((2, far), (1, after), (3, back))):
        loads += rows_of(w, where_x, block, to, [sems.at[CHUNKS + 2 * j], sems.at[CHUNKS + 2 * j + 1]])
    for load in loads:
        load.start()

    @pl.loop(0, CHUNKS)
    def _(k):
        pltpu.make_async_copy(up.at[k], up.at[k], sems.at[k]).wait()
        got = jnp.maximum(dot(xn[...], up[k].reshape(2048, 512), 1, 0), 0.0)
        hidden[:, pl.ds(pl.multiple_of(k * 512, 512), 512)] = (got * got).astype(BF)

    for load in loads[CHUNKS : CHUNKS + 2]:
        load.wait()
    down_body(hidden, far, top, bottom)
    for load in loads[CHUNKS + 2 :]:
        load.wait()


def own_body(where_x, h, source, top, bottom, w, sems):
    loads = rows_of(source, where_x, 0, w, [sems.at[0], sems.at[1]])
    for load in loads:
        load.start()
    for load in loads:
        load.wait()
    down_body(h, w, top, bottom)


def down_body(h, w, top, bottom):
    got = dot(h[:, 0:1024], w[:, 0].reshape(512, 1024), 1, 1)
    got = (got + dot(h[:, 1024:2048], w[:, 1].reshape(512, 1024), 1, 1)).astype(BF)
    top[...] = got[0:QUARTER]
    bottom[...] = got[QUARTER:]


def join_body(a, b, c, d, left, right):
    left[...] = (a[...].astype(F32) + b[...].astype(F32)).astype(BF)
    right[...] = (c[...].astype(F32) + d[...].astype(F32)).astype(BF)


def second_body(resid, own_top, own_bottom, top1, bottom1, top3, bottom3, second, stats):
    top = own_top[...].astype(F32) + top1[...].astype(F32) + top3[...].astype(F32)
    bottom = own_bottom[...].astype(F32) + bottom1[...].astype(F32) + bottom3[...].astype(F32)
    total = RES * resid[...].astype(F32) + jnp.concatenate([top, bottom], axis=0)
    second[...] = total
    s1 = jnp.transpose(jnp.broadcast_to(jnp.sum(total, axis=1, keepdims=True), (HALF, 128)))[0:8, :]
    s2 = jnp.transpose(jnp.broadcast_to(jnp.sum(total * total, axis=1, keepdims=True), (HALF, 128)))[0:8, :]
    stats[...] = jnp.where(iota((8, HALF), 0) == 0, s1, s2)


def last_body(core, second, s0, s1, s2, s3, gain_a, gain_b, full, send):
    stats = s0[...] + s1[...] + s2[...] + s3[...]
    cols = jnp.transpose(stats)
    m = cols[:, 0:1] / 2048.0
    v = cols[:, 1:2] / 2048.0 - m * m
    scale = lax.rsqrt(v + EPS)
    mine = pl.multiple_of(core[0] * 256, 256)
    other = pl.multiple_of(256 - core[0] * 256, 256)
    send[...] = ((second[:, pl.ds(other, 256)] - m) * scale * gain_b[1:2, :]).astype(BF)
    rows = pl.ds(pl.multiple_of(core[0] * HALF, HALF), HALF)
    full[rows, :] = ((second[:, pl.ds(mine, 256)] - m) * scale * gain_a[1:2, :]).astype(BF)


def layer(
    head_value_rows,
    entry_map_rows,
    readout_map_rows,
    output_gate_rows,
    step_before_softplus,
    sudden_log_decay,
    document_index,
    head_rate_logarithm,
    head_step_bias,
    value_conv_taps,
    entry_conv_taps,
    readout_conv_taps,
    group_norm_gain,
    mixer_output_weight,
    stream,
    mixer_norm_gain,
    channel_norm_gain,
    up_projection_weight,
    down_projection_weight,
):
    core = lax.axis_index("c")
    at_x = jnp.reshape(lax.axis_index("x"), (1,))
    at_c = jnp.reshape(core, (1,))
    at_y = jnp.reshape(lax.axis_index("y"), (1,))
    at_sp = jnp.reshape(lax.axis_index(SP), (1,))
    swap = [(0, 1), (1, 0)]

    def shift(a, axis, by, count):
        return lax.ppermute(a, axis, [(i, i + by) for i in range(count) if 0 <= i + by < count])

    def around(a, by):
        return lax.ppermute(a, "x", [(i, (i + by) % 4) for i in range(4)])

    tail = jnp.concatenate([a[ROWS - 2 :] for a in (head_value_rows, entry_map_rows, readout_map_rows)], axis=1)
    head = jnp.concatenate([a[:2] for a in (head_value_rows, entry_map_rows, readout_map_rows)], axis=1)
    low = shift(tail, SP, 1, 32)
    high = shift(head, SP, -1, 32)

    weights = jnp.concatenate([up_projection_weight, down_projection_weight], axis=1)
    weights = lax.all_gather(weights, ("z", "y", "c"), axis=0, tiled=True).reshape(32, 2, 64, 2048)

    weight_other = lax.ppermute(mixer_output_weight, "c", swap)
    stream_mine = lax.dynamic_slice_in_dim(stream, core * HALF, HALF)
    stream_other = lax.ppermute(lax.dynamic_slice_in_dim(stream, (1 - core) * HALF, HALF), "c", swap)
    gains = jnp.stack([mixer_norm_gain, channel_norm_gain])
    gains_other = lax.ppermute(gains, "c", swap)

    x, b, c, cum, dt, ct, dev, doc, si, pay = call(
        conv_body,
        14,
        [((ROWS, 256), BF), ((ROWS, 128), BF), ((ROWS, 128), BF)]
        + [((8, ROWS), F32)] * 5
        + [((6, 128, 256), BF), ((144, 512), BF)],
        scratch=[pltpu.VMEM((784, 512), F32)],
        scalars=3,
        far=(1, 2, 3, 4, 5, 8, 9, 10, 13),
    )(
        at_sp, head_rate_logarithm, head_step_bias, head_value_rows, entry_map_rows, readout_map_rows,
        low, high, value_conv_taps, entry_conv_taps, readout_conv_taps, step_before_softplus,
        sudden_log_decay, document_index.reshape(192, 128),
    )
    rows = lax.all_gather(pay, "y")
    send_f, send_b, pre = call(
        chain_body, 2, [((144, 256), BF), ((144, 256), BF), ((136, 512), F32)], scalars=1
    )(at_y, rows)
    f1, f2 = shift(send_f, "z", 1, 8), shift(send_f, "z", 2, 8)
    b1, b2 = shift(send_b, "z", -1, 8), shift(send_b, "z", -2, 8)
    yl = call(local_body, 8, [((ROWS, 256), F32)])(x, b, c, cum, dt, ct, doc, si)[0]
    keep, send = call(
        gate_body, 11, [((HALF, 256), BF)] * 2, scratch=[pltpu.VMEM((ROWS, 256), BF)], scalars=1, far=(9, 10)
    )(at_c, yl, c, dev, pre, f1, f2, b1, b2, output_gate_rows, group_norm_gain.reshape(1, 256))
    other = lax.ppermute(send, "c", swap)
    o0, o1, o2, o3 = call(mix_body, 5, [((HALF, 512), BF)] * 4, scalars=1, far=(3,))(
        at_x, keep, other, mixer_output_weight, weight_other
    )
    r2, r1, r3 = around(o2, 2), around(o1, 1), around(o3, 3)
    top, bottom = call(
        first_body,
        9,
        [((QUARTER, 512), BF), ((QUARTER + 16, 512), BF)],
        scratch=[pltpu.VMEM((HALF, 512), F32), pltpu.VMEM((8, 512), F32)],
        scalars=1,
    )(at_c, o0, stream_mine, stream_other, r1, r2, r3, gains, gains_other)
    top1, bottom3 = around(top, 1), around(bottom, 3)
    top3, bottom1 = around(top, 3), around(bottom, 1)
    top2, bottom2 = around(top1, 1), around(bottom3, 3)
    rows, resid = call(rows_body, 9, [((HALF, 2048), BF), ((HALF, 512), BF)], scalars=1)(
        at_x, top, bottom, top1, bottom1, top2, bottom2, top3, bottom3
    )
    hidden, part1, part3, far_top, far_bottom = pl.pallas_call(
        up_body,
        in_specs=[sm(), vm(), pl.BlockSpec(memory_space=pltpu.HBM)],
        out_specs=[vm()] * 5,
        out_shape=[pltpu.VMEM((HALF, 2048), BF)]
        + [pltpu.VMEM((8, 2, 64, 1024), BF)] * 2
        + [pltpu.VMEM((QUARTER, 512), BF)] * 2,
        scratch_shapes=[
            pltpu.VMEM((8, 2, 64, 1024), BF),
            pltpu.VMEM((CHUNKS, 32, 64, 2048 // CHUNKS), BF),
            pltpu.SemaphoreType.DMA((CHUNKS + 6,)),
        ],
        compiler_params=pltpu.CompilerParams(vmem_limit_bytes=32 * 2**20),
        name="up",
    )(at_x, near(rows), off(weights))

    def down(part):
        return call(down_body, 2, [((QUARTER, 512), BF)] * 2)(hidden, part)

    far_top, far_bottom = around(far_top, 1), around(far_bottom, 3)
    next_top, next_bottom = down(part1)
    next_bottom = around(next_bottom, 1)
    back_top, back_bottom = down(part3)
    back_top = around(back_top, 3)
    own_top, own_bottom = pl.pallas_call(
        own_body,
        in_specs=[sm(), vm(), pl.BlockSpec(memory_space=pltpu.HBM)],
        out_specs=[vm()] * 2,
        out_shape=[pltpu.VMEM((QUARTER, 512), BF)] * 2,
        scratch_shapes=[pltpu.VMEM((8, 2, 64, 1024), BF), pltpu.SemaphoreType.DMA((2,))],
        compiler_params=pltpu.CompilerParams(vmem_limit_bytes=24 * 2**20),
        name="down0",
    )(at_x, near(hidden), off(weights))
    next_top, back_bottom = call(join_body, 4, [((QUARTER, 512), BF)] * 2)(next_top, far_top, back_bottom, far_bottom)
    next_top, back_bottom = around(next_top, 1), around(back_bottom, 3)
    second, stats = call(second_body, 7, [((HALF, 512), F32), ((8, HALF), F32)])(
        resid, own_top, own_bottom, next_top, next_bottom, back_top, back_bottom
    )
    s1, s2, s3 = around(stats, 1), around(stats, 2), around(stats, 3)
    full, send = call(last_body, 8, [((ROWS, 256), BF), ((HALF, 256), BF)], scalars=1, plain=(0,))(
        at_c, second, stats, s1, s2, s3, gains, gains_other
    )
    got = lax.ppermute(send, "c", swap)
    return lax.dynamic_update_slice_in_dim(full, got, (1 - core) * HALF, 0)


def solution(mesh):
    torus = Mesh(mesh.devices.reshape(8, 4, 4, 2), ("z", "y", "x", "c"))
    return jax.shard_map(
        layer,
        mesh=torus,
        in_specs=(
            P(SP, TP),
            P(SP, TP),
            P(SP, TP),
            P(SP, TP),
            P(SP, TP),
            P(SP, TP),
            P(),
            P(None, TP),
            P(None, TP),
            P(None, TP),
            P(None, TP),
            P(None, TP),
            P(TP),
            P(TP, None),
            P(SP, TP),
            P(TP),
            P(TP),
            P(SP, TP),
            P(SP, TP),
        ),
        out_specs=P(SP, TP),
        check_vma=False,
    )
```
